32 devices in a mesh: ep: 8 (over z, y), tp: 4 (over x, core).
Axes of the slice: x: 2, y: 2, z: 4, core: 2. Of those that a mesh axis runs over, the one named last changes fastest.
Arguments:
- tokens: bfloat16 [128, 2048], P('ep'), may hold values from -6 to 6
- norm_gain: bfloat16 [2048], replicated, may hold values from 0.099609375 to 1.8984375
- query_weight: bfloat16 [2048, 1024], P('ep', 'tp'), may hold values from -0.125 to 0.125
- key_weight: bfloat16 [2048, 1024], P('ep', 'tp'), may hold values from -0.125 to 0.125
- value_weight: bfloat16 [2048, 2048], P('ep', 'tp'), may hold values from -0.125 to 0.125
- outgate_weight: bfloat16 [2048, 2048], P('ep', 'tp'), may hold values from -0.125 to 0.125
- beta_weight: bfloat16 [2048, 16], replicated, may hold values from -0.125 to 0.125
- decay_weight: bfloat16 [2048, 16], replicated, may hold values from -0.125 to 0.125
- decay_rate: float32 [16], P('tp'), may hold values from 0.02 to 6
- decay_bias: float32 [16], P('tp'), may hold values from -3 to 3
- head_gain: bfloat16 [128], replicated, may hold values from 0.099609375 to 1.8984375
- recurrent: float32 [128, 16, 128, 128], P('ep', 'tp'), may hold values from -3 to 3
- output_weight: bfloat16 [2048, 2048], P('tp', 'ep'), may hold values from -0.125 to 0.125
- ffn_gain: bfloat16 [2048], replicated, may hold values from 0.099609375 to 1.8984375
- routes: int32 [128, 4], P('ep'), may hold values from 0 to 7, all different within a row; in each aligned block of 16 rows (0 to 15, 16 to 31, ...) at most 16 rows name the same one
- route_weight: float32 [128, 4], P('ep'), may hold values from 0.1 to 1
- expert_gate: bfloat16 [8, 2048, 512], P('ep', None, 'tp'), may hold values from -0.125 to 0.125
- expert_up: bfloat16 [8, 2048, 512], P('ep', None, 'tp'), may hold values from -0.125 to 0.125
- expert_down: bfloat16 [8, 512, 2048], P('ep', 'tp'), may hold values from -0.25 to 0.25
- shared_gate: bfloat16 [2048, 512], P('ep', 'tp'), may hold values from -0.125 to 0.125
- shared_up: bfloat16 [2048, 512], P('ep', 'tp'), may hold values from -0.125 to 0.125
- shared_down: bfloat16 [512, 2048], P('tp', 'ep'), may hold values from -0.25 to 0.25
- branch_gate: bfloat16 [2048], replicated, may hold values from -0.125 to 0.125
Outputs:
- layer_out: bfloat16 [128, 2048], P('ep')
- new_state: float32 [128, 16, 128, 128], P('ep', 'tp')
The draws below stay inside these ranges and needn't reach their ends.
Inputs may be any that keep to these rules, and one draw needn't show every extreme that they name: `routes`: each row names 4 different experts. Among the rows of one aligned block of 16 rows no expert is named more than 16 times, and some block reaches it: one expert is named exactly 16 times there.
All inputs are finite; a program needn't handle non-finite values.
Results may differ from the reference program's by a relative error of at most 0.019.
Values may be sent and summed in bfloat16 or wider, within the bound.
A program may use at most 64 MiB of HBM per device.

```python
import math
import jax
import jax.numpy as jnp
import numpy as np
from jax import lax

D = 2048
DK = 128
DV = 128
HK = 8
HV = 16
D_EXPERT = 512
D_SHARED = 512
TOPK = 4
SEQ_DEV = 16
SEQS = 128
EXPERTS = 8
CAP = 16
N_EP = 8
N_TP = 4


def levels(stream_key, dims, shards, smallest, high):
    def one(position, blocks):
        draws = jax.random.uniform(jax.random.fold_in(jax.random.fold_in(stream_key, 6), position), (blocks,), jnp.float32, smallest / len(shards), high / len(shards))
        return jnp.repeat(jnp.exp(draws), dims[position] // blocks).reshape((-1,) + (1,) * (len(dims) - position - 1))

    level = one(*shards[0])
    for cut in shards[1:]:
        level = level * one(*cut)
    return level


def routed_block(stream_key, own, number, rows, number_of, top, most, slope):
    sequence = jax.random.permutation(stream_key, number_of)
    heavy_load, ordinary = shares(number_of, rows * top, most, slope, True), shares(number_of, rows * top, most, slope, False)
    places = jnp.arange(number_of)

    def named(sizes, turn):
        used = int((sizes > 0).sum())
        fixed = max(1, used // 4)
        shifted = fixed + (places - fixed + turn * (used - fixed)) % max(1, number_of - fixed)
        return jnp.zeros((number_of,), jnp.int32).at[sequence[jnp.where(places < fixed, places, shifted)]].set(jnp.asarray(sizes, jnp.int32))

    sizes = jnp.where(number % 4 == 0, named(heavy_load, number // 4), named(ordinary, number - number // 4 - 1))
    mixed = jax.random.permutation(jax.random.fold_in(own, 3), number_of)
    source_of, taker = mixed[0:number_of // 2 * 2:2], mixed[1:number_of // 2 * 2:2]
    margin = jnp.minimum(sizes[source_of] - 1, most - sizes[taker]) // 2
    margin = jnp.where((source_of == sequence[0]) | (taker == sequence[0]) | (sizes[taker] == 0), 0, jnp.maximum(margin, 0))
    shifted = jax.random.randint(jax.random.fold_in(own, 4), (number_of // 2,), 0, 1 << 20) % (margin + 1)
    sizes = sizes.at[source_of].add(-shifted).at[taker].add(shifted)
    items = jnp.searchsorted(jnp.cumsum(sizes), jnp.arange(rows * top), side="right").astype(jnp.int32)
    table = items.reshape(top, rows).T
    table = table[jax.random.permutation(jax.random.fold_in(own, 1), rows)]
    turn = jax.random.randint(jax.random.fold_in(own, 2), (rows, 1), 0, top)
    return jnp.take_along_axis(table, (jnp.arange(top)[None, :] + turn) % top, axis=1)


def shares(count, total, most, lean, full):
    loads = [(1 << 20) // math.isqrt(standing ** lean) + 1 for standing in range(1, count + 1)]
    largest = most if full else min(most, max(-(-total // count), total * loads[0] // sum(loads)))
    least = 1 if total - largest >= count - 1 else 0
    given, rest = [largest] + [least] * (count - 1), total - largest - least * (count - 1)
    while rest > 0:
        free = [i for i in range(1, count) if given[i] < largest] or [i for i in range(1, count) if given[i] < most]
        pool, left = sum([loads[i] for i in free]), rest
        for i in free:
            extra = min(most - given[i], max(1, left * loads[i] // pool), rest)
            given[i] = given[i] + extra
            rest = rest - extra
    return np.array(given)


def noise(stream_key, extent, deviation, reach, pieces=(), held_as=jnp.bfloat16):
    values = jax.random.normal(stream_key, extent, jnp.float32) * deviation
    if len(pieces) > 0:
        values = levels(stream_key, extent, pieces, -0.22, 0.18) * values
    return jnp.clip(values, min=-reach, max=reach).astype(held_as)


def setup_inputs(seed: int = 0) -> dict:
    key_of = jax.random.split(jax.random.key(seed), 24)
    tokens = noise(key_of[0], (SEQS, D), 1.0, 6.0, ((0, 8),))
    norm_gain = jnp.clip(1.0 + 0.18 * jax.random.normal(key_of[1], (D,), jnp.float32), 0.099609375, 1.8984375).astype(jnp.bfloat16)
    query_weight = noise(key_of[2], (D, HK * DK), D ** -0.5, 0.125, ((0, 8), (1, 4)))
    key_weight = noise(key_of[3], (D, HK * DK), D ** -0.5, 0.125, ((0, 8), (1, 4)))
    value_weight = noise(key_of[4], (D, HV * DV), D ** -0.5, 0.125, ((0, 8), (1, 4)))
    outgate_weight = noise(key_of[5], (D, HV * DV), D ** -0.5, 0.125, ((0, 8), (1, 4)))
    beta_weight = noise(key_of[6], (D, HV), D ** -0.5, 0.125)
    decay_weight = noise(key_of[7], (D, HV), D ** -0.5, 0.125)
    decay_rate = jnp.clip(jnp.exp(math.log(6.0) - 5.7037825 * jax.random.uniform(key_of[8], (HV,), jnp.float32) ** levels(key_of[8], (HV,), ((0, 4),), -0.2, 0.2)), 0.02, 6.0)
    decay_bias = noise(key_of[9], (HV,), 1.0, 3.0, ((0, 4),), jnp.float32)
    head_gain = jnp.clip(1.0 + 0.18 * jax.random.normal(key_of[10], (DV,), jnp.float32), 0.099609375, 1.8984375).astype(jnp.bfloat16)
    recurrent = noise(key_of[11], (SEQS, HV, DK, DV), 0.5, 3.0, ((0, 8), (1, 4)), jnp.float32)
    output_weight = noise(key_of[12], (HV * DV, D), (HV * DV) ** -0.5, 0.125, ((0, 4), (1, 8)))
    ffn_gain = jnp.clip(1.0 + 0.18 * jax.random.normal(key_of[13], (D,), jnp.float32), 0.099609375, 1.8984375).astype(jnp.bfloat16)
    routes_keys = jax.random.split(jax.random.fold_in(key_of[14], 1), SEQS // SEQ_DEV)
    routes_turns = jax.random.permutation(jax.random.fold_in(key_of[14], 3), SEQS // SEQ_DEV)
    routes = jax.vmap(lambda own, number: routed_block(jax.random.fold_in(key_of[14], 2), own, number, SEQ_DEV, EXPERTS, TOPK, CAP, 2))(routes_keys, routes_turns).reshape((SEQS, TOPK))
    route_weight = jnp.clip(jnp.exp(math.log(1.0) - 2.3025851 * jax.random.uniform(key_of[15], (SEQS, TOPK), jnp.float32) ** levels(key_of[15], (SEQS, TOPK), ((0, 8),), -0.2, 0.2)), 0.1, 1.0)
    expert_gate = noise(key_of[16], (EXPERTS, D, D_EXPERT), D ** -0.5, 0.125, ((0, 8), (2, 4)))
    expert_up = noise(key_of[17], (EXPERTS, D, D_EXPERT), D ** -0.5, 0.125, ((0, 8), (2, 4)))
    expert_down = noise(key_of[18], (EXPERTS, D_EXPERT, D), D_EXPERT ** -0.5, 0.25, ((0, 8), (1, 4)))
    shared_gate = noise(key_of[19], (D, D_SHARED), D ** -0.5, 0.125, ((0, 8), (1, 4)))
    shared_up = noise(key_of[20], (D, D_SHARED), D ** -0.5, 0.125, ((0, 8), (1, 4)))
    shared_down = noise(key_of[21], (D_SHARED, D), D_SHARED ** -0.5, 0.25, ((0, 4), (1, 8)))
    branch_gate = noise(key_of[22], (D,), D ** -0.5, 0.125)
    return dict(tokens=tokens, norm_gain=norm_gain, query_weight=query_weight, key_weight=key_weight, value_weight=value_weight, outgate_weight=outgate_weight, beta_weight=beta_weight, decay_weight=decay_weight, decay_rate=decay_rate, decay_bias=decay_bias, head_gain=head_gain, recurrent=recurrent, output_weight=output_weight, ffn_gain=ffn_gain, routes=routes, route_weight=route_weight, expert_gate=expert_gate, expert_up=expert_up, expert_down=expert_down, shared_gate=shared_gate, shared_up=shared_up, shared_down=shared_down, branch_gate=branch_gate)


EPS = 1e-06
ROUTED_SCALE = 2.5

def rms_scale(values, gain):
    values = values.astype(jnp.float32)
    return values * lax.rsqrt(lax.optimization_barrier(jnp.mean(values * values, axis=-1, keepdims=True)) + EPS) * gain.astype(jnp.float32)

def unit_rows(values):
    return values * lax.rsqrt(lax.optimization_barrier(jnp.sum(values * values, axis=-1, keepdims=True)) + EPS)

def grouped_product(left, right, groups):
    inner = left.shape[1] // groups
    running = jnp.zeros((left.shape[0], right.shape[1]), jnp.float32)
    for index in range(groups):
        partial_product = jnp.dot(left[:, index * inner:(index + 1) * inner], right[index * inner:(index + 1) * inner], preferred_element_type=jnp.float32)
        running = running + partial_product.astype(jnp.bfloat16).astype(jnp.float32)
    return running

def reference(tokens, norm_gain, query_weight, key_weight, value_weight, outgate_weight, beta_weight, decay_weight, decay_rate, decay_bias, head_gain, recurrent, output_weight, ffn_gain, routes, route_weight, expert_gate, expert_up, expert_down, shared_gate, shared_up, shared_down, branch_gate):
    seqs, width = tokens.shape
    heads, key_dim, value_dim = (recurrent.shape[1], recurrent.shape[2], recurrent.shape[3])
    key_heads = query_weight.shape[1] // key_dim
    normed = rms_scale(tokens, norm_gain).astype(jnp.bfloat16)
    query_proj = jnp.dot(normed, query_weight, preferred_element_type=jnp.float32).astype(jnp.bfloat16)
    key_proj = jnp.dot(normed, key_weight, preferred_element_type=jnp.float32).astype(jnp.bfloat16)
    value_proj = jnp.dot(normed, value_weight, preferred_element_type=jnp.float32).astype(jnp.bfloat16)
    gate_proj = jnp.dot(normed, outgate_weight, preferred_element_type=jnp.float32).astype(jnp.bfloat16)
    beta_logit = jnp.dot(normed, beta_weight, preferred_element_type=jnp.float32)
    decay_logit = jnp.dot(normed, decay_weight, preferred_element_type=jnp.float32)
    repeat_count = heads // key_heads
    queries = unit_rows(jax.nn.silu(query_proj.astype(jnp.float32)).reshape(seqs, key_heads, key_dim))
    queries = jnp.repeat(queries, repeat_count, axis=1) * key_dim ** (-0.5)
    key_rows = unit_rows(jax.nn.silu(key_proj.astype(jnp.float32)).reshape(seqs, key_heads, key_dim))
    key_rows = jnp.repeat(key_rows, repeat_count, axis=1)
    value_rows = jax.nn.silu(value_proj.astype(jnp.float32)).reshape(seqs, heads, value_dim)
    strength = jax.nn.sigmoid(beta_logit)
    retain = jnp.exp(-decay_rate[None, :] * jax.nn.softplus(decay_logit + decay_bias[None, :]))
    decayed = recurrent * retain[:, :, None, None]
    predicted = jnp.einsum('shde,shd->she', decayed, key_rows, precision=lax.Precision.HIGHEST)
    correction = strength[:, :, None] * (value_rows - predicted)
    new_state = decayed + key_rows[:, :, :, None] * correction[:, :, None, :]
    readout = jnp.einsum('shde,shd->she', new_state, queries, precision=lax.Precision.HIGHEST)
    out_gate = jax.nn.silu(gate_proj.astype(jnp.float32)).reshape(seqs, heads, value_dim)
    heads_out = (rms_scale(readout, head_gain) * out_gate).astype(jnp.bfloat16).reshape(seqs, heads * value_dim)
    mix = grouped_product(heads_out, output_weight, N_TP)
    residual = (tokens.astype(jnp.float32) + mix).astype(jnp.bfloat16)
    ffn_in = rms_scale(residual, ffn_gain).astype(jnp.bfloat16)
    topk = routes.shape[1]
    seq_local = seqs // N_EP
    experts_total = expert_gate.shape[0]
    pair_count = seq_local * topk
    pair_ids = routes.reshape(N_EP, pair_count).astype(jnp.int32)
    onehot = (pair_ids[:, :, None] == jnp.arange(experts_total).astype(jnp.int32)[None, None, :]).astype(jnp.int32)
    slots = lax.optimization_barrier(jnp.sum((jnp.cumsum(onehot, axis=1) - onehot) * onehot, axis=2)).astype(jnp.int32)
    target = (pair_ids * CAP + slots).astype(jnp.int32)
    source_rows = jnp.repeat(ffn_in.reshape(N_EP, seq_local, width), topk, axis=1)
    buffer = jnp.zeros((N_EP, experts_total * CAP, width), jnp.bfloat16)
    source_index = jnp.arange(N_EP).astype(jnp.int32)[:, None]
    buffer = buffer.at[source_index, target].set(source_rows)
    buffer = buffer.reshape(N_EP, experts_total, CAP, width).transpose(1, 0, 2, 3).reshape(experts_total, N_EP * CAP, width)

    def expert_rows(operands):
        rows_in, gate_matrix, up_matrix, down_matrix = operands
        gate_part = jnp.dot(rows_in, gate_matrix, preferred_element_type=jnp.float32)
        up_part = jnp.dot(rows_in, up_matrix, preferred_element_type=jnp.float32)
        act = (jax.nn.silu(gate_part) * up_part).astype(jnp.bfloat16)
        return grouped_product(act, down_matrix, N_TP).astype(jnp.bfloat16)
    results = lax.map(expert_rows, (buffer, expert_gate, expert_up, expert_down))
    results = results.reshape(experts_total, N_EP, CAP, width).transpose(1, 0, 2, 3).reshape(N_EP, experts_total * CAP, width)
    pair_out = jnp.take_along_axis(results, target[:, :, None], axis=1).astype(jnp.float32)
    scaled = route_weight / lax.optimization_barrier(jnp.sum(route_weight, axis=1, keepdims=True)) * ROUTED_SCALE
    moe = lax.optimization_barrier(jnp.sum(pair_out.reshape(seqs, topk, width) * scaled[:, :, None], axis=1))
    shared_g = jnp.dot(ffn_in, shared_gate, preferred_element_type=jnp.float32)
    shared_u = jnp.dot(ffn_in, shared_up, preferred_element_type=jnp.float32)
    shared_act = (jax.nn.silu(shared_g) * shared_u).astype(jnp.bfloat16)
    shared_out = grouped_product(shared_act, shared_down, N_TP)
    branch = jax.nn.sigmoid(jnp.dot(ffn_in, branch_gate, preferred_element_type=jnp.float32))
    layer_out = (residual.astype(jnp.float32) + moe + branch[:, None] * shared_out).astype(jnp.bfloat16)
    return (layer_out, new_state)
```

```python
import functools
import types

import jax
import jax.numpy as jnp
from jax import lax
from jax.experimental import pallas as pl
from jax.experimental.pallas import tpu as pltpu
from jax.sharding import PartitionSpec as P

EPS = 1e-06
ROUTED_SCALE = 2.5
MESH = pl.DeviceIdType.MESH
F32 = jnp.float32
BF16 = jnp.bfloat16
STATE_PARTS = 4


def silu(v):
    return v / (1.0 + jnp.exp(-v))


def sigmoid(v):
    return 1.0 / (1.0 + jnp.exp(-v))


def rms_scale(values, gain):
    values = values.astype(F32)
    return (
        values
        * lax.rsqrt(jnp.mean(values * values, axis=-1, keepdims=True) + EPS)
        * gain.astype(F32).reshape(1, -1)
    )


def unit_rows(values):
    return values * lax.rsqrt(jnp.sum(values * values, axis=-1, keepdims=True) + EPS)


def dot(a, b):
    return jnp.dot(a, b, preferred_element_type=F32)


def dot_nt(a, b):
    return lax.dot_general(a, b, (((1,), (1,)), ((), ())), preferred_element_type=F32)


def remote(src, dst, send_sem, recv_sem, e, t):
    return pltpu.make_async_remote_copy(
        src_ref=src,
        dst_ref=dst,
        send_sem=send_sem,
        recv_sem=recv_sem,
        device_id=(e, t),
        device_id_type=MESH,
    )


def loop(lo, hi, body):
    def step(i, c):
        body(i)
        return c

    lax.fori_loop(lo, hi, step, 0)


def layer_kernel(n, m, names, *refs):
    r = types.SimpleNamespace(**dict(zip(names, refs)))
    me, tp = lax.axis_index("ep"), lax.axis_index("tp")
    count = n * m
    lin = me * m + tp
    half = m // 2
    group = n // m
    core = lax.rem(tp, 2)
    pair = tp + 1 - 2 * core
    xi = tp // 2
    rows, width = r.tokens.shape
    depth, qc = r.qw_hbm.shape
    vc = r.vw_hbm.shape[1]
    key_dim, value_dim = r.new.shape[2], r.new.shape[3]
    heads = r.new.shape[1]
    keys = qc // key_dim
    near = 2 * qc + vc
    cols = r.ow.shape[1]
    hidden = r.eg_hbm.shape[2]
    quarter = width // m
    units = r.ssend.shape[1] // 3
    mates = half * group
    tall = mates * rows

    fetches = {}

    def fetch(name, src, dst):
        c = pltpu.make_async_copy(src, dst, r.wsem.at[len(fetches)])
        c.start()
        fetches[name] = c

    for name in ("tokens", "gain", "sg", "su", "sd", "beta", "decay", "rate", "bias"):
        fetch(name, getattr(r, name + "_hbm"), getattr(r, name))
    at = 0
    for name in ("qw", "kw", "vw", "gw"):
        src = getattr(r, name + "_hbm")
        fetch(name, src, r.weights.at[:, pl.ds(at, src.shape[1])])
        at += src.shape[1]
    for name in ("routes", "rw", "head_gain", "ffn_gain", "bg"):
        fetch(name, getattr(r, name + "_hbm"), getattr(r, name))
    part = rows // STATE_PARTS
    for i in range(STATE_PARTS):
        these = pl.ds(i * part, part)
        fetch(("state", i), r.state_hbm.at[these], r.new.at[these])
    fetch("ow", r.ow_hbm, r.ow)
    mine = pl.ds(pl.multiple_of(core * hidden, hidden), hidden)
    fetch("eg", r.eg_hbm.at[0], r.eg.at[:, mine])
    fetch("eu", r.eu_hbm.at[0], r.eu.at[:, mine])
    fetch("ed", r.ed_hbm.at[0], r.ed.at[mine])

    barrier = pltpu.get_barrier_semaphore()

    def greet(i):
        p = lax.rem(lin + i, count)
        pl.semaphore_signal(
            barrier, inc=1, device_id=(p // m, lax.rem(p, m)), device_id_type=MESH
        )

    loop(1, count, greet)

    fetches["tokens"].wait()
    fetches["gain"].wait()
    tokens = r.tokens[...]
    normed = rms_scale(tokens, r.gain[...]).astype(BF16)
    for e in range(n):
        r.xsend[e] = normed[:, e * depth : (e + 1) * depth]
        r.tsend[e] = tokens[:, e * depth : (e + 1) * depth]
    for at, name in enumerate(("sg", "su", "sd")):
        fetches[name].wait()
        w = getattr(r, name)[...]
        by_unit = w if at == 2 else w.astype(F32).T.astype(BF16)
        for e in range(n):
            r.ssend[e, at * units : (at + 1) * units] = by_unit[e * units : (e + 1) * units]
    pl.semaphore_wait(barrier, count - 1)

    def x_copy(i):
        p = lax.rem(me + i, n)
        return remote(r.xsend.at[p], r.xbuf.at[me], r.xs.at[i], r.xr.at[me], p, tp)

    loop(1, n, lambda i: x_copy(i).start())
    r.xbuf[me] = r.xsend[me]

    def s_copy(i):
        p = lax.rem(me + i, n)
        return remote(r.ssend.at[p], r.sbuf.at[core, me], r.ss.at[i], r.sr.at[me], p, tp)

    loop(1, n, lambda i: s_copy(i).start())
    r.sbuf[core, me] = r.ssend[me]

    e_copies = [
        remote(r.eg_hbm.at[0], r.eg.at[:, mine], r.es.at[0], r.er.at[0], me, pair),
        remote(r.eu_hbm.at[0], r.eu.at[:, mine], r.es.at[1], r.er.at[1], me, pair),
        remote(r.ed_hbm.at[0], r.ed.at[mine], r.es.at[2], r.er.at[2], me, pair),
    ]
    for c in e_copies:
        c.start()

    for name in ("beta", "decay", "rate", "bias", "routes", "rw"):
        fetches[name].wait()
    column = lax.broadcasted_iota(jnp.int32, (rows, r.beta.shape[0]), 1)

    def own_heads(w):
        logits = dot_nt(normed, w)
        return [
            jnp.sum(jnp.where(column == tp * heads + h, logits, 0.0), axis=1, keepdims=True)
            for h in range(heads)
        ]

    def wide(v):
        return jnp.broadcast_to(v, (rows, value_dim))

    beta = own_heads(r.beta[...])
    decay = own_heads(r.decay[...])
    strengths = []
    for h in range(heads):
        at = slice(h * value_dim, (h + 1) * value_dim)
        strength = sigmoid(wide(beta[h]))
        shifted = wide(decay[h]) + r.bias[:, h : h + 1]
        softplus = jnp.maximum(shifted, 0.0) + jnp.log1p(jnp.exp(-jnp.abs(shifted)))
        retain = jnp.exp(-r.rate[:, h : h + 1] * softplus)
        r.retain[:, at] = retain
        r.pull[:, at] = strength * retain
        strengths.append(strength)
    rw = r.rw[...]
    scaled = rw / jnp.sum(rw, axis=0, keepdims=True) * ROUTED_SCALE
    routes = r.routes[...]
    expert = lax.broadcasted_iota(jnp.int32, (128, rows), 0)
    by_expert = jnp.zeros((128, rows), F32)
    for k in range(routes.shape[0]):
        by_expert = by_expert + jnp.where(
            expert == routes[k : k + 1, :], scaled[k : k + 1, :], 0.0
        )
    by_expert = by_expert.T
    lane = lax.broadcasted_iota(jnp.int32, (rows, 128), 1)
    for e in range(n):
        w = by_expert[:, e : e + 1]
        high = w.astype(BF16).astype(F32)
        r.bsend[e, :, vc:] = jnp.where(lane < 64, high, w - high).astype(BF16)

    for name in ("qw", "kw", "vw", "gw"):
        fetches[name].wait()

    def got_x(i):
        p = lax.rem(me + i, n)
        remote(r.xbuf.at[p], r.xbuf.at[p], r.xs.at[i], r.xr.at[p], p, tp).wait_recv()

    loop(1, n, got_x)
    x = r.xbuf[...].reshape(n * rows, depth)

    def project(lo, hi, to):
        step = 512
        for c in range(lo, hi, step):
            size = min(step, hi - c)
            out = dot(x, r.weights[:, c : c + size])
            to[:, :, c - lo : c - lo + size] = out.astype(BF16).reshape(n, rows, size)

    def a_copy(i):
        p = lax.rem(me + i, n)
        return remote(r.asend.at[p], r.abuf.at[me], r.as_.at[i], r.ar.at[me], p, tp)

    def b_copy(i):
        p = lax.rem(me + i, n)
        return remote(r.bsend.at[p], r.bbuf.at[me], r.bs.at[i], r.br.at[me], p, tp)

    project(0, near, r.asend)
    loop(1, n, lambda i: a_copy(i).start())
    project(near, near + vc, r.bsend)
    loop(1, n, lambda i: b_copy(i).start())
    r.abuf[me] = r.asend[me]
    r.bbuf[me] = r.bsend[me]

    def t_copy(i):
        p = lax.rem(me + i, n)
        at = lax.rem(me, group)
        return remote(r.tsend.at[p], r.tbuf.at[at], r.ts.at[i], r.tr.at[at], p, tp)

    @pl.when(tp == me // group)
    def _():
        loop(1, n, lambda i: t_copy(i).start())
        r.tbuf[lax.rem(me, group)] = r.tsend[me]

    def s_pass(i):
        p = lax.rem(me + i, n)
        ref = r.sbuf.at[core, p]
        return remote(ref, ref, r.s2s.at[i], r.s2r.at[p], me, pair)

    def got_s(i):
        p = lax.rem(me + i, n)
        ref = r.sbuf.at[core, p]
        remote(ref, ref, r.ss.at[i], r.sr.at[p], p, tp).wait_recv()
        s_pass(i).start()

    s_pass(0).start()
    loop(1, n, got_s)

    def got_a(i):
        p = lax.rem(me + i, n)
        remote(r.abuf.at[p], r.abuf.at[p], r.as_.at[i], r.ar.at[p], p, tp).wait_recv()

    loop(1, n, got_a)

    def gathered(ref, c, size):
        acc = ref[0, :, c : c + size].astype(F32)
        for e in range(1, n):
            acc = acc + ref[e, :, c : c + size].astype(F32)
        return acc.astype(BF16).astype(F32)

    q_rows = [
        unit_rows(silu(gathered(r.abuf, j * key_dim, key_dim))) * key_dim ** (-0.5)
        for j in range(keys)
    ]
    k_rows = [
        unit_rows(silu(gathered(r.abuf, qc + j * key_dim, key_dim))) for j in range(keys)
    ]
    for h in range(heads):
        at = slice(h * value_dim, (h + 1) * value_dim)
        r.push[:, at] = strengths[h] * silu(
            gathered(r.abuf, 2 * qc + h * value_dim, value_dim)
        )
    for j in range(keys):
        r.qk[:, j * value_dim : (j + 1) * value_dim] = wide(
            jnp.sum(q_rows[j] * k_rows[j], axis=1, keepdims=True)
        )
    stacked = q_rows + k_rows
    stacked.append(jnp.zeros((128 - 2 * keys * rows, key_dim), F32))
    r.kq[...] = jnp.concatenate(stacked, axis=0).T
    for i in range(STATE_PARTS):
        fetches[("state", i)].wait()
    fetches["head_gain"].wait()

    share = heads // keys

    def h_copy(j, i):
        p = lax.rem(me + i, n)
        ref = r.hbuf.at[j, me]
        return remote(ref, ref, r.hs.at[j, i], r.hr.at[j, me], p, tp)

    def got_b(i):
        p = lax.rem(me + i, n)
        remote(r.bbuf.at[p], r.bbuf.at[p], r.bs.at[i], r.br.at[p], p, tp).wait_recv()

    for j in range(keys):

        for s in range(rows):
            q = jnp.broadcast_to(r.kq[:, j * rows + s : j * rows + s + 1], (key_dim, value_dim))
            at = (keys + j) * rows + s
            k = jnp.broadcast_to(r.kq[:, at : at + 1], (key_dim, value_dim))
            one = slice(s, s + 1)
            qk = r.qk[one, j * value_dim : (j + 1) * value_dim]
            for h in range(j * share, (j + 1) * share):
                c = slice(h * value_dim, (h + 1) * value_dim)
                state = r.new[s, h]
                retain = r.retain[one, c]
                predicted = jnp.sum(state * k, axis=0, keepdims=True)
                before = jnp.sum(state * q, axis=0, keepdims=True)
                correction = r.push[one, c] - r.pull[one, c] * predicted
                r.new[s, h] = state * retain + k * correction
                r.held[one, c] = before * retain + qk * correction

        if j == 0:
            loop(1, n, got_b)
        for h in range(j * share, (j + 1) * share):
            c = slice(h * value_dim, (h + 1) * value_dim)
            at = (h - j * share) * value_dim
            gate = silu(gathered(r.bbuf, h * value_dim, value_dim))
            r.hbuf[j, me, :, at : at + value_dim] = (
                rms_scale(r.held[:, c], r.head_gain[...]) * gate
            ).astype(BF16)
        loop(1, n, functools.partial(lambda j, i: h_copy(j, i).start(), j))

    for a in range(half):
        for b in range(group):
            e = (2 * a + core) * group + b
            w = r.bbuf[e, :, vc:].astype(F32)
            at = (a * group + b) * rows
            r.routed[at : at + rows] = jnp.broadcast_to(
                w[:, 0:1] + w[:, 64:65], (rows, 128)
            )

    def got_s2(i):
        p = lax.rem(me + i, n)
        ref = r.sbuf.at[1 - core, p]
        remote(ref, ref, r.s2s.at[i], r.s2r.at[p], me, pair).wait_recv()

    loop(0, n, got_s2)
    for c in range(2):
        r.shared[c] = jnp.concatenate([r.sbuf[c, e] for e in range(n)], axis=1)
    fetches["ow"].wait()

    def got_h(j, i):
        p = lax.rem(me + i, n)
        ref = r.hbuf.at[j, p]
        remote(ref, ref, r.hs.at[j, i], r.hr.at[j, p], p, tp).wait_recv()

    chunk = share * value_dim
    mix = None
    for j in range(keys):
        loop(1, n, functools.partial(got_h, j))
        term = dot(r.hbuf[j].reshape(n * rows, chunk), r.ow[j * chunk : (j + 1) * chunk])
        mix = term if mix is None else mix + term
    r.msend[...] = mix.astype(BF16).reshape(m, group * rows, cols)

    def m_copy(i):
        t = lax.rem(tp + i, m)
        return remote(r.msend.at[t], r.mbuf.at[tp], r.ms.at[i], r.mr.at[tp], me, t)

    loop(1, m, lambda i: m_copy(i).start())
    r.mbuf[tp] = r.msend[tp]

    def got_t(a):
        e = tp * group + a

        @pl.when(e != me)
        def _():
            remote(r.tbuf.at[a], r.tbuf.at[a], r.ts.at[0], r.tr.at[a], e, tp).wait_recv()

    loop(0, group, got_t)

    def got_m(i):
        t = lax.rem(tp + i, m)
        remote(r.mbuf.at[t], r.mbuf.at[t], r.ms.at[i], r.mr.at[t], me, t).wait_recv()

    loop(1, m, got_m)
    acc = r.mbuf[0].astype(F32)
    for t in range(1, m):
        acc = acc + r.mbuf[t].astype(F32)
    residual = (r.tbuf[...].reshape(group * rows, cols).astype(F32) + acc).astype(BF16)
    r.resid[xi, me] = residual.reshape(group, rows, cols)

    def f_copy(i):
        p = lax.rem(me + i, n)
        ref = r.resid.at[xi, me]
        return remote(ref, ref, r.fs.at[i], r.fr.at[me], p, tp)

    def f_pass(i, k):
        p = lax.rem(me + n - i, n)
        ref = r.resid.at[xi, p]
        t = 2 * lax.rem(xi + k, half) + core
        return remote(ref, ref, r.gs.at[k, i], r.gr.at[xi, p], me, t)

    loop(1, n, lambda i: f_copy(i).start())
    for k in range(1, half):
        f_pass(0, k).start()

    def got_f(i):
        p = lax.rem(me + n - i, n)
        ref = r.resid.at[xi, p]
        remote(ref, ref, r.fs.at[i], r.fr.at[p], p, tp).wait_recv()
        for k in range(1, half):
            f_pass(i, k).start()

    loop(1, n, got_f)
    for name in ("ffn_gain", "bg", "eg", "eu", "ed"):
        fetches[name].wait()
    for i, ref in enumerate((r.eg.at[:, pl.ds(pl.multiple_of((1 - core) * hidden, hidden), hidden)],
                             r.eu.at[:, pl.ds(pl.multiple_of((1 - core) * hidden, hidden), hidden)],
                             r.ed.at[pl.ds(pl.multiple_of((1 - core) * hidden, hidden), hidden)])):
        remote(ref, ref, r.es.at[i], r.er.at[i], me, pair).wait_recv()

    def got_g(i):
        p = lax.rem(me + n - i, n)
        for k in range(1, half):
            a = lax.rem(xi + k, half)
            ref = r.resid.at[a, p]
            remote(ref, ref, r.gs.at[k, i], r.gr.at[a, p], me, 2 * a + core).wait_recv()

    loop(0, n, got_g)

    owner = me // group
    held_here = core == lax.rem(owner, 2)
    place, which = owner // 2, lax.rem(me, group)

    def d_copy():
        return remote(
            r.resid.at[place, pl.ds(pair * group, group), which],
            r.rown,
            r.ds.at[0],
            r.dr.at[0],
            me,
            pair,
        )

    @pl.when(held_here)
    def _():
        d_copy().start()
        r.rown[...] = r.resid[place, pl.ds(tp * group, group), which]

    blocks = [r.resid[:, e].reshape(tall, cols).astype(F32) for e in range(n)]
    square = blocks[0] * blocks[0]
    for b in blocks[1:]:
        square = square + b * b
    scale = lax.rsqrt(jnp.sum(square, axis=1, keepdims=True) / width + EPS)
    gain = r.ffn_gain[...].astype(F32).reshape(1, -1)
    ffn = jnp.concatenate(
        [
            (b * scale * gain[:, e * cols : (e + 1) * cols]).astype(BF16)
            for e, b in enumerate(blocks)
        ],
        axis=1,
    )
    act = (silu(dot(ffn, r.eg[...])) * dot(ffn, r.eu[...])).astype(BF16)
    shared_acts = []
    for c in range(2):
        both = dot_nt(ffn, r.shared[c, : 2 * units])
        shared_acts.append((silu(both[:, :units]) * both[:, units:]).astype(BF16))
    bg = r.bg[...].astype(F32).reshape(1, -1)
    branch = sigmoid(jnp.sum(ffn.astype(F32) * bg, axis=1, keepdims=True))
    weight = r.routed[:, 0:1]

    def target(s):
        return (2 * (s // group) + core) * group + lax.rem(s, group)

    def r_copy(s, q):
        return remote(
            r.rsend.at[s, q],
            r.rbuf.at[me * half + xi],
            r.rs.at[s, q],
            r.rr.at[me * half + xi],
            target(s),
            q,
        )

    def away(s, q):
        return jnp.logical_or(target(s) != me, q != tp)

    first = lax.rem(me, mates)
    for k in range(m):
        q = lax.rem(tp + k, m)
        at = pl.ds(pl.multiple_of(q * quarter, quarter), quarter)
        out = weight * dot(act, r.ed[:, at])
        side = dot(shared_acts[0], r.shared[0, 2 * units :, at])
        side = side + dot(shared_acts[1], r.shared[1, 2 * units :, at])
        r.rsend[:, q] = (out + branch * side).astype(BF16).reshape(mates, rows, quarter)

        def send_r(i, q=q):
            s = lax.rem(first + i, mates)

            @pl.when(away(s, q))
            def _():
                r_copy(s, q).start()

        loop(0, mates, send_r)

    @pl.when(held_here)
    def _():
        r.rbuf[me * half + xi] = r.rsend[place * group + which, tp]

    def got_r(i):
        p = lax.rem(me + i // half, n)
        a = lax.rem(xi + i, half)
        t = 2 * a + lax.rem(owner, 2)
        ref = r.rbuf.at[p * half + a]

        @pl.when(jnp.logical_or(p != me, t != tp))
        def _():
            remote(ref, ref, r.rs.at[0, 0], r.rr.at[p * half + a], p, t).wait_recv()

    loop(0, n * half, got_r)

    @pl.when(jnp.logical_not(held_here))
    def _():
        remote(r.rown, r.rown, r.ds.at[0], r.dr.at[0], me, pair).wait_recv()

    acc = jnp.concatenate([r.rown[b].astype(F32) for b in range(group)], axis=1)
    for p in range(n * half):
        acc = acc + r.rbuf[p].astype(F32)
    r.obuf[tp] = acc.astype(BF16)

    def o_copy(i):
        t = lax.rem(tp + i, m)
        return remote(r.obuf.at[tp], r.obuf.at[tp], r.os_.at[i], r.or_.at[tp], me, t)

    loop(1, m, lambda i: o_copy(i).start())

    def left_ep(i):
        x_copy(i).wait_send()
        s_copy(i).wait_send()
        a_copy(i).wait_send()
        b_copy(i).wait_send()
        f_copy(i).wait_send()
        for j in range(keys):
            h_copy(j, i).wait_send()

    loop(1, n, left_ep)

    def left_pass(i):
        s_pass(i).wait_send()
        for k in range(1, half):
            f_pass(i, k).wait_send()

    loop(0, n, left_pass)

    @pl.when(tp == me // group)
    def _():
        loop(1, n, lambda i: t_copy(i).wait_send())

    @pl.when(held_here)
    def _():
        d_copy().wait_send()

    for c in e_copies:
        c.wait_send()
    loop(1, m, lambda i: m_copy(i).wait_send())

    def left_r(i):
        s, q = i // m, lax.rem(i, m)

        @pl.when(away(s, q))
        def _():
            r_copy(s, q).wait_send()

    loop(0, mates * m, left_r)

    def got_o(i):
        t = lax.rem(tp + i, m)
        ref = r.obuf.at[t]
        remote(ref, ref, r.os_.at[i], r.or_.at[t], me, t).wait_recv()

    loop(1, m, got_o)
    for t in range(m):
        r.out[:, t * quarter : (t + 1) * quarter] = r.obuf[t]
    loop(1, m, lambda i: o_copy(i).wait_send())


def flush_kernel(layer_ref, state_ref, layer_out, state_out, sem):
    rows = state_ref.shape[0]
    part = rows // STATE_PARTS
    copies = [pltpu.make_async_copy(layer_ref, layer_out, sem.at[STATE_PARTS])]
    for i in range(STATE_PARTS):
        these = pl.ds(i * part, part)
        copies.append(
            pltpu.make_async_copy(state_ref.at[these], state_out.at[these], sem.at[i])
        )
    for c in copies:
        c.start()
    for c in copies:
        c.wait()


VMEM = pl.BlockSpec(memory_space=pltpu.VMEM)
HBM = pl.BlockSpec(memory_space=pltpu.HBM)


def per_device(
    n,
    m,
    tokens,
    norm_gain,
    query_weight,
    key_weight,
    value_weight,
    outgate_weight,
    beta_weight,
    decay_weight,
    decay_rate,
    decay_bias,
    head_gain,
    recurrent,
    output_weight,
    ffn_gain,
    routes,
    route_weight,
    expert_gate,
    expert_up,
    expert_down,
    shared_gate,
    shared_up,
    shared_down,
    branch_gate,
):
    rows, width = tokens.shape
    _, heads, key_dim, value_dim = recurrent.shape
    depth, qc = query_weight.shape
    vc = value_weight.shape[1]
    keys = qc // key_dim
    near = 2 * qc + vc
    half = m // 2
    group = n // m
    mates = half * group
    units = shared_gate.shape[1] // n
    cols = shared_down.shape[1]
    hidden = expert_gate.shape[2]
    quarter = width // m
    sds = jax.ShapeDtypeStruct
    dma = pltpu.SemaphoreType.DMA

    inputs = dict(
        tokens=tokens,
        gain=norm_gain,
        qw=query_weight,
        kw=key_weight,
        vw=value_weight,
        gw=outgate_weight,
        beta=beta_weight.T,
        decay=decay_weight.T,
        rate=decay_rate[None, :],
        bias=decay_bias[None, :],
        routes=routes.T,
        rw=route_weight.T,
        head_gain=head_gain,
        state=recurrent,
        ow=output_weight,
        ffn_gain=ffn_gain,
        eg=expert_gate,
        eu=expert_up,
        ed=expert_down,
        sg=shared_gate,
        su=shared_up,
        sd=shared_down,
        bg=branch_gate,
    )
    plain = ("tokens", "gain", "beta", "decay", "rate", "bias", "routes", "rw")
    plain += ("head_gain", "ffn_gain", "sg", "su", "sd", "bg", "ow")
    scratch = {k: pltpu.VMEM(inputs[k].shape, inputs[k].dtype) for k in plain}
    scratch.update(
        weights=pltpu.VMEM((depth, near + vc), BF16),
        eg=pltpu.VMEM((width, 2 * hidden), BF16),
        eu=pltpu.VMEM((width, 2 * hidden), BF16),
        ed=pltpu.VMEM((2 * hidden, width), BF16),
        xsend=pltpu.VMEM((n, rows, depth), BF16),
        xbuf=pltpu.VMEM((n, rows, depth), BF16),
        tsend=pltpu.VMEM((n, rows, depth), BF16),
        tbuf=pltpu.VMEM((group, rows, depth), BF16),
        ssend=pltpu.VMEM((n, 3 * units, cols), BF16),
        sbuf=pltpu.VMEM((2, n, 3 * units, cols), BF16),
        shared=pltpu.VMEM((2, 3 * units, width), BF16),
        asend=pltpu.VMEM((n, rows, near), BF16),
        abuf=pltpu.VMEM((n, rows, near), BF16),
        bsend=pltpu.VMEM((n, rows, vc + 128), BF16),
        bbuf=pltpu.VMEM((n, rows, vc + 128), BF16),
        retain=pltpu.VMEM((rows, vc), F32),
        pull=pltpu.VMEM((rows, vc), F32),
        push=pltpu.VMEM((rows, vc), F32),
        qk=pltpu.VMEM((rows, keys * value_dim), F32),
        kq=pltpu.VMEM((key_dim, 128), F32),
        held=pltpu.VMEM((rows, vc), F32),
        routed=pltpu.VMEM((mates * rows, 128), F32),
        hbuf=pltpu.VMEM((keys, n, rows, vc // keys), BF16),
        msend=pltpu.VMEM((m, group * rows, cols), BF16),
        mbuf=pltpu.VMEM((m, group * rows, cols), BF16),
        resid=pltpu.VMEM((half, n, group, rows, cols), BF16),
        rown=pltpu.VMEM((group, rows, cols), BF16),
        rsend=pltpu.VMEM((mates, m, rows, quarter), BF16),
        rbuf=pltpu.VMEM((n * half, rows, quarter), BF16),
        obuf=pltpu.VMEM((m, rows, quarter), BF16),
        wsem=dma((len(inputs) + STATE_PARTS,)),
        xs=dma((n,)),
        xr=dma((n,)),
        ss=dma((n,)),
        sr=dma((n,)),
        s2s=dma((n,)),
        s2r=dma((n,)),
        as_=dma((n,)),
        ar=dma((n,)),
        bs=dma((n,)),
        br=dma((n,)),
        ts=dma((n,)),
        tr=dma((group,)),
        hs=dma((keys, n)),
        hr=dma((keys, n)),
        ms=dma((m,)),
        mr=dma((m,)),
        fs=dma((n,)),
        fr=dma((n,)),
        gs=dma((half, n)),
        gr=dma((half, n)),
        es=dma((3,)),
        er=dma((3,)),
        ds=dma((1,)),
        dr=dma((1,)),
        rs=dma((mates, m)),
        rr=dma((n * half,)),
        os_=dma((m,)),
        or_=dma((m,)),
    )
    names = [k + "_hbm" for k in inputs] + ["out", "new"] + list(scratch)
    layer, state = pl.pallas_call(
        functools.partial(layer_kernel, n, m, names),
        out_shape=(pltpu.VMEM((rows, width), BF16), pltpu.VMEM(recurrent.shape, F32)),
        in_specs=[HBM] * len(inputs),
        out_specs=(VMEM, VMEM),
        scratch_shapes=list(scratch.values()),
        compiler_params=pltpu.CompilerParams(
            collective_id=0, has_side_effects=True, vmem_limit_bytes=48 * 2**20
        ),
    )(*(pltpu.with_memory_space_constraint(v, pltpu.HBM) for v in inputs.values()))

    return pl.pallas_call(
        flush_kernel,
        out_shape=(sds((rows, width), BF16), sds(recurrent.shape, F32)),
        in_specs=[VMEM, VMEM],
        out_specs=(HBM, HBM),
        scratch_shapes=[dma((STATE_PARTS + 1,))],
        compiler_params=pltpu.CompilerParams(vmem_limit_bytes=4 * 2**20),
    )(layer, state)


def solution(mesh):
    return jax.shard_map(
        functools.partial(per_device, mesh.shape["ep"], mesh.shape["tp"]),
        mesh=mesh,
        in_specs=(
            P("ep", None),
            P(),
            P("ep", "tp"),
            P("ep", "tp"),
            P("ep", "tp"),
            P("ep", "tp"),
            P(),
            P(),
            P("tp"),
            P("tp"),
            P(),
            P("ep", "tp", None, None),
            P("tp", "ep"),
            P(),
            P("ep", None),
            P("ep", None),
            P("ep", None, "tp"),
            P("ep", None, "tp"),
            P("ep", "tp", None),
            P("ep", "tp"),
            P("ep", "tp"),
            P("tp", "ep"),
            P(),
        ),
        out_specs=(P("ep", None), P("ep", "tp", None, None)),
        check_vma=False,
    )
```

```python
import functools
import types

import jax
import jax.numpy as jnp
from jax import lax
from jax.experimental import pallas as pl
from jax.experimental.pallas import tpu as pltpu
from jax.sharding import PartitionSpec as P

EPS = 1e-06
ROUTED_SCALE = 2.5
MESH = pl.DeviceIdType.MESH
F32 = jnp.float32
BF16 = jnp.bfloat16
STATE_PARTS = 4


def silu(v):
    return v / (1.0 + jnp.exp(-v))


def sigmoid(v):
    return 1.0 / (1.0 + jnp.exp(-v))


def rms_scale(values, gain):
    values = values.astype(F32)
    return (
        values
        * lax.rsqrt(jnp.mean(values * values, axis=-1, keepdims=True) + EPS)
        * gain.astype(F32).reshape(1, -1)
    )


def unit_rows(values):
    return values * lax.rsqrt(jnp.sum(values * values, axis=-1, keepdims=True) + EPS)


def dot(a, b):
    return jnp.dot(a, b, preferred_element_type=F32)


def dot_nt(a, b):
    return lax.dot_general(a, b, (((1,), (1,)), ((), ())), preferred_element_type=F32)


def remote(src, dst, send_sem, recv_sem, e, t):
    return pltpu.make_async_remote_copy(
        src_ref=src,
        dst_ref=dst,
        send_sem=send_sem,
        recv_sem=recv_sem,
        device_id=(e, t),
        device_id_type=MESH,
    )


def loop(lo, hi, body):
    def step(i, c):
        body(i)
        return c

    lax.fori_loop(lo, hi, step, 0)


def layer_kernel(n, m, names, *refs):
    r = types.SimpleNamespace(**dict(zip(names, refs)))
    me, tp = lax.axis_index("ep"), lax.axis_index("tp")
    count = n * m
    lin = me * m + tp
    half = m // 2
    group = n // m
    core = lax.rem(tp, 2)
    pair = tp + 1 - 2 * core
    xi = tp // 2
    home = lax.rem(me, m)
    turn = me // m
    rows, width = r.tokens.shape
    depth, qc = r.qw_hbm.shape
    vc = r.vw_hbm.shape[1]
    key_dim, value_dim = r.new.shape[2], r.new.shape[3]
    heads = r.new.shape[1]
    keys = qc // key_dim
    share = heads // keys
    near = 2 * qc + vc
    cols = r.wide_ow.shape[1]
    hidden = r.eg_hbm.shape[2]
    quarter = width // m
    units = r.ssend2.shape[1]
    tall = group * rows

    barrier = pltpu.get_barrier_semaphore()

    def greet(i):
        p = lax.rem(lin + i, count)
        pl.semaphore_signal(
            barrier, inc=1, device_id=(p // m, lax.rem(p, m)), device_id_type=MESH
        )

    loop(1, count, greet)

    fetches, alone = {}, []

    def fetch(name, src, dst, sem=None):
        if sem is None:
            sem = r.wsem.at[len(alone)]
            alone.append(name)
        c = pltpu.make_async_copy(src, dst, sem)
        c.start()
        fetches[name] = c

    for name in ("tokens", "gain"):
        fetch(name, getattr(r, name + "_hbm"), getattr(r, name))
    at = 0
    for name in ("qw", "kw", "vw", "gw"):
        src = getattr(r, name + "_hbm")
        fetch(name, src, r.weights.at[:, pl.ds(at, src.shape[1])], r.psem.at[0])
        at += src.shape[1]
    for name in ("routes", "rw", "beta", "decay", "rate", "bias", "sg", "su", "sd"):
        fetch(name, getattr(r, name + "_hbm"), getattr(r, name))
    part = rows // STATE_PARTS
    for i in range(STATE_PARTS):
        these = pl.ds(i * part, part)
        fetch(("state", i), r.state_hbm.at[these], r.new.at[these], r.psem.at[1])
    for name in ("head_gain", "ffn_gain", "bg"):
        fetch(name, getattr(r, name + "_hbm"), getattr(r, name))
    own_ow = pl.ds(pl.multiple_of(tp * vc, vc), vc)
    mine = pl.ds(pl.multiple_of(core * hidden, hidden), hidden)
    other = pl.ds(pl.multiple_of((1 - core) * hidden, hidden), hidden)
    fetch("ow", r.ow_hbm, r.wide_ow.at[own_ow])
    fetch("eg", r.eg_hbm.at[0], r.eg.at[:, mine])
    fetch("eu", r.eu_hbm.at[0], r.eu.at[:, mine])
    fetch("ed", r.ed_hbm.at[0], r.ed.at[mine])

    steps = [
        (1 - 2 * lax.rem(me // 2**i, 2)) * 2**i for i in range(n.bit_length() - 1)
    ]

    def peer(k):
        p = me
        for i, step in enumerate(steps):
            if k >> i & 1:
                p = p + step
        return p

    cuts = (n // 2, 3 * n // 4, n), (n // 4, n // 2), (0, n // 4)
    spans = [cuts[0][:2], cuts[0][1:], cuts[1], cuts[2]]
    order = [k for lo, hi in spans for k in range(lo, hi) if k]

    def arrived(ref, sem):
        remote(ref, ref, sem, sem, me, pair).wait_recv()

    def left(ref, sem):
        remote(ref, ref, sem, sem, me, pair).wait_send()

    fetches["tokens"].wait()
    fetches["gain"].wait()
    tokens = r.tokens[...]
    normed = rms_scale(tokens, r.gain[...]).astype(BF16)
    for e in range(n):
        r.xsend[e] = normed[:, e * depth : (e + 1) * depth]
        r.tsend[e] = tokens[:, e * depth : (e + 1) * depth]

    fetches["routes"].wait()
    fetches["rw"].wait()
    rw = r.rw[...]
    scaled = rw / jnp.sum(rw, axis=0, keepdims=True) * ROUTED_SCALE
    routes = r.routes[...]
    expert = lax.broadcasted_iota(jnp.int32, (128, rows), 0)
    by_expert = jnp.zeros((128, rows), F32)
    for k in range(routes.shape[0]):
        by_expert = by_expert + jnp.where(
            expert == routes[k : k + 1, :], scaled[k : k + 1, :], 0.0
        )
    by_expert = by_expert.T
    lane = lax.broadcasted_iota(jnp.int32, (rows, 128), 1)
    for e in range(n):
        w = by_expert[:, e : e + 1]
        high = w.astype(BF16).astype(F32)
        r.csend[e] = jnp.where(lane < 64, high, w - high).astype(BF16)
    pl.semaphore_wait(barrier, count - 1)

    for g, (lo, hi) in enumerate(spans):
        for k in range(max(lo, 1), hi):
            p = peer(k)
            remote(r.xsend.at[p], r.xbuf.at[k], r.xs.at[0], r.xr.at[g], p, tp).start()
    r.xbuf[0] = r.xsend[me]
    for k in order:
        p = peer(k)
        remote(r.csend.at[p], r.cbuf.at[me], r.cs.at[0], r.cr.at[0], p, tp).start()
    r.cbuf[me] = r.csend[me]

    for i in range(1, m):
        t = lax.rem(tp + i, m)
        remote(r.ow_hbm, r.wide_ow.at[own_ow], r.ows.at[0], r.owr.at[0], me, t).start()
    e_copies = [
        remote(r.eg_hbm.at[0], r.eg.at[:, mine], r.es.at[0], r.er.at[0], me, pair),
        remote(r.eu_hbm.at[0], r.eu.at[:, mine], r.es.at[1], r.er.at[1], me, pair),
        remote(r.ed_hbm.at[0], r.ed.at[mine], r.es.at[2], r.er.at[2], me, pair),
    ]
    for c in e_copies:
        c.start()

    for name in ("beta", "decay", "rate", "bias", "sg", "su", "sd"):
        fetches[name].wait()
    column = lax.broadcasted_iota(jnp.int32, (rows, r.beta.shape[0]), 1)

    def own_heads(w):
        logits = dot_nt(normed, w)
        return [
            jnp.sum(jnp.where(column == tp * heads + h, logits, 0.0), axis=1, keepdims=True)
            for h in range(heads)
        ]

    def wide(v):
        return jnp.broadcast_to(v, (rows, value_dim))

    beta = own_heads(r.beta[...])
    decay = own_heads(r.decay[...])
    for h in range(heads):
        at = slice(h * value_dim, (h + 1) * value_dim)
        strength = sigmoid(wide(beta[h]))
        shifted = wide(decay[h]) + r.bias[:, h : h + 1]
        softplus = jnp.maximum(shifted, 0.0) + jnp.log1p(jnp.exp(-jnp.abs(shifted)))
        retain = jnp.exp(-r.rate[:, h : h + 1] * softplus)
        r.retain[:, at] = retain
        r.pull[:, at] = strength * retain
        r.push[:, at] = strength
    for at, name in enumerate(("sg", "su")):
        by_unit = getattr(r, name)[...].astype(F32).T.astype(BF16)
        for e in range(n):
            r.ssend1[e, at * units : (at + 1) * units] = by_unit[e * units : (e + 1) * units]
    for e in range(n):
        r.ssend2[e] = r.sd[e * units : (e + 1) * units]

    pltpu.make_async_copy(r.weights, r.weights, r.psem.at[0]).wait()
    for g, (lo, hi) in enumerate(spans):
        if hi > max(lo, 1):
            arrived(r.xbuf.at[pl.ds(max(lo, 1), hi - max(lo, 1))], r.xr.at[g])
        x = r.xbuf[lo:hi].reshape((hi - lo) * rows, depth)
        for c in range(0, near, 512):
            size = min(512, near - c)
            out = dot(x, r.weights[:, c : c + size])
            r.asend[lo:hi, :, c : c + size] = out.astype(BF16).reshape(hi - lo, rows, size)
        for k in range(max(lo, 1), hi):
            remote(
                r.asend.at[k], r.abuf.at[k], r.as_.at[0], r.ar.at[0], peer(k), tp
            ).start()
    r.abuf[0] = r.asend[0]
    x = r.xbuf[...].reshape(n * rows, depth)
    out = dot(x, r.weights[:, near:])
    r.bsend[...] = out.astype(BF16).reshape(n, rows, vc)
    for k in order:
        remote(r.bsend.at[k], r.bbuf.at[k], r.bs.at[0], r.br.at[0], peer(k), tp).start()
    r.bbuf[0] = r.bsend[0]

    at_home = tp == home

    @pl.when(at_home)
    def _():
        for k in order:
            p = peer(k)
            remote(
                r.tsend.at[p], r.tbuf.at[turn], r.ts.at[0], r.tr.at[0], p, tp
            ).start()
        r.tbuf[turn] = r.tsend[me]

    def send_shared(src, dst, s, d):
        for k in order:
            p = peer(k)
            remote(src.at[p], dst.at[core, me], s.at[0], d.at[0], p, tp).start()
        dst[core, me] = src[me]

    send_shared(r.ssend1, r.sbuf1, r.s1s, r.s1r)

    arrived(r.cbuf.at[pl.ds(0, n - 1)], r.cr.at[0])
    for a in range(half):
        for b in range(group):
            w = r.cbuf[b * m + 2 * a + core].astype(F32)
            r.routed[a, b * rows : (b + 1) * rows] = jnp.broadcast_to(
                w[:, 0:1] + w[:, 64:65], (rows, 128)
            )
    fetches["head_gain"].wait()
    pltpu.make_async_copy(r.new, r.new, r.psem.at[1]).wait()

    arrived(r.abuf.at[pl.ds(1, n - 1)], r.ar.at[0])

    def gathered(ref, c, size):
        acc = ref[0, :, c : c + size].astype(F32)
        for e in range(1, n):
            acc = acc + ref[e, :, c : c + size].astype(F32)
        return acc.astype(BF16).astype(F32)

    q_rows = [
        unit_rows(silu(gathered(r.abuf, j * key_dim, key_dim))) * key_dim ** (-0.5)
        for j in range(keys)
    ]
    k_rows = [
        unit_rows(silu(gathered(r.abuf, qc + j * key_dim, key_dim))) for j in range(keys)
    ]
    for h in range(heads):
        at = slice(h * value_dim, (h + 1) * value_dim)
        r.push[:, at] = r.push[:, at] * silu(
            gathered(r.abuf, 2 * qc + h * value_dim, value_dim)
        )
    for j in range(keys):
        r.qk[:, j * value_dim : (j + 1) * value_dim] = wide(
            jnp.sum(q_rows[j] * k_rows[j], axis=1, keepdims=True)
        )
    stacked = q_rows + k_rows
    stacked.append(jnp.zeros((128 - 2 * keys * rows, key_dim), F32))
    r.kq[...] = jnp.concatenate(stacked, axis=0).T

    for j in range(keys):
        for s in range(rows):
            q = jnp.broadcast_to(r.kq[:, j * rows + s : j * rows + s + 1], (key_dim, value_dim))
            at = (keys + j) * rows + s
            k = jnp.broadcast_to(r.kq[:, at : at + 1], (key_dim, value_dim))
            one = slice(s, s + 1)
            qk = r.qk[one, j * value_dim : (j + 1) * value_dim]
            for h in range(j * share, (j + 1) * share):
                c = slice(h * value_dim, (h + 1) * value_dim)
                state = r.new[s, h]
                retain = r.retain[one, c]
                predicted = jnp.sum(state * k, axis=0, keepdims=True)
                before = jnp.sum(state * q, axis=0, keepdims=True)
                correction = r.push[one, c] - r.pull[one, c] * predicted
                r.new[s, h] = state * retain + k * correction
                r.held[one, c] = before * retain + qk * correction

    arrived(r.bbuf.at[pl.ds(1, n - 1)], r.br.at[0])
    for h in range(heads):
        c = slice(h * value_dim, (h + 1) * value_dim)
        gate = silu(gathered(r.bbuf, h * value_dim, value_dim))
        r.hsend[:, c] = (rms_scale(r.held[:, c], r.head_gain[...]) * gate).astype(BF16)

    def send_h(p):
        remote(
            r.hsend, r.hbuf.at[turn * m + tp], r.hs.at[0], r.hr.at[0], p, home
        ).start()

    for k in order:
        send_h(peer(k))

    @pl.when(jnp.logical_not(at_home))
    def _():
        send_h(me)

    @pl.when(at_home)
    def _():
        r.hbuf[turn * m + tp] = r.hsend[...]

    send_shared(r.ssend2, r.sbuf2, r.s2s, r.s2r)

    fetches["ow"].wait()
    arrived(r.wide_ow.at[pl.ds(0, (m - 1) * vc)], r.owr.at[0])

    @pl.when(at_home)
    def _():
        arrived(r.tbuf.at[pl.ds(0, group - 1)], r.tr.at[0])
        arrived(r.hbuf.at[pl.ds(0, n - 1)], r.hr.at[0])

    @pl.when(jnp.logical_not(at_home))
    def _():
        arrived(r.tbuf, r.tr.at[0])
        arrived(r.hbuf, r.hr.at[0])

    residual = r.tbuf[...].reshape(tall, cols).astype(F32)
    mix = None
    for t in range(m):
        h = jnp.concatenate([r.hbuf[b * m + t] for b in range(group)], axis=0)
        term = dot(h, r.wide_ow[t * vc : (t + 1) * vc])
        mix = term if mix is None else mix + term
    r.resid[xi, me] = (residual + mix).astype(BF16).reshape(group, rows, cols)

    mine_resid = r.resid.at[xi, me]
    for k in order:
        remote(mine_resid, mine_resid, r.fs.at[0], r.fr.at[k], peer(k), tp).start()

    def f_pass(p):
        ref = r.resid.at[xi, p]
        for i in range(1, half):
            t = 2 * lax.rem(xi + i, half) + core
            remote(ref, ref, r.gs.at[0], r.gr.at[xi], me, t).start()

    f_pass(me)
    arrived(r.sbuf1.at[0, pl.ds(0, n - 1)], r.s1r.at[0])
    s_copies = [remote(r.sbuf1.at[core], r.sbuf1.at[core], r.ps.at[0], r.pr.at[0], me, pair)]
    s_copies[0].start()
    arrived(r.sbuf2.at[0, pl.ds(0, n - 1)], r.s2r.at[0])
    s_copies.append(
        remote(r.sbuf2.at[core], r.sbuf2.at[core], r.ps.at[1], r.pr.at[1], me, pair)
    )
    s_copies[1].start()
    for k in order:
        p = peer(k)
        arrived(r.resid.at[xi, p], r.fr.at[k])
        f_pass(p)
    arrived(r.sbuf1.at[0], r.pr.at[0])
    arrived(r.sbuf2.at[0], r.pr.at[1])
    for c in range(2):
        r.shared[c, : 2 * units] = jnp.concatenate([r.sbuf1[c, e] for e in range(n)], axis=1)
        r.shared[c, 2 * units :] = jnp.concatenate([r.sbuf2[c, e] for e in range(n)], axis=1)
    for name in ("ffn_gain", "bg", "eg", "eu", "ed"):
        fetches[name].wait()
    for i, ref in enumerate((r.eg.at[:, other], r.eu.at[:, other], r.ed.at[other])):
        arrived(ref, r.er.at[i])

    gain = r.ffn_gain[...].astype(F32).reshape(1, -1)
    bg = r.bg[...].astype(F32).reshape(1, -1)
    upper = me // (n // 2)

    def target(a, b):
        return b * m + 2 * a + core

    def away(a, b, q):
        return jnp.logical_or(target(a, b) != me, q != tp)

    def work(a):
        blocks = [r.resid[a, e].reshape(tall, cols).astype(F32) for e in range(n)]
        square = blocks[0] * blocks[0]
        for v in blocks[1:]:
            square = square + v * v
        scale = lax.rsqrt(jnp.sum(square, axis=1, keepdims=True) / width + EPS)
        ffn = jnp.concatenate(
            [
                (v * scale * gain[:, e * cols : (e + 1) * cols]).astype(BF16)
                for e, v in enumerate(blocks)
            ],
            axis=1,
        )
        act = (silu(dot(ffn, r.eg[...])) * dot(ffn, r.eu[...])).astype(BF16)
        dense = []
        for c in range(2):
            both = dot_nt(ffn, r.shared[c, : 2 * units])
            dense.append((silu(both[:, :units]) * both[:, units:]).astype(BF16))
        branch = sigmoid(jnp.sum(ffn.astype(F32) * bg, axis=1, keepdims=True))
        weight = r.routed[a, :, 0:1]
        for k in range(m):
            q = lax.rem(tp + k, m)
            at = pl.ds(pl.multiple_of(q * quarter, quarter), quarter)
            out = weight * dot(act, r.ed[:, at])
            side = dot(dense[0], r.shared[0, 2 * units :, at])
            side = side + dot(dense[1], r.shared[1, 2 * units :, at])
            r.rsend[a, :, q] = (out + branch * side).astype(BF16).reshape(group, rows, quarter)
            for i in range(group):
                b = lax.rem(i + (group // 2) * (1 - upper), group)

                @pl.when(away(a, b, q))
                def _():
                    remote(
                        r.rsend.at[a, b, q],
                        r.rbuf.at[me * half + xi],
                        r.rs.at[0],
                        r.rr.at[0],
                        target(a, b),
                        q,
                    ).start()

    work(xi)
    for i in range(1, half):
        a = lax.rem(xi + i, half)
        arrived(r.resid.at[a], r.gr.at[a])
        work(a)

    held_here = core == lax.rem(home, 2)
    place = home // 2
    d_copy = remote(
        r.resid.at[place, pl.ds(pair * group, group), turn],
        r.rown,
        r.ds.at[0],
        r.dr.at[0],
        me,
        pair,
    )

    @pl.when(held_here)
    def _():
        d_copy.start()
        r.rown[...] = r.resid[place, pl.ds(tp * group, group), turn]
        r.rbuf[me * half + xi] = r.rsend[place, turn, tp]

    left(r.xbuf.at[pl.ds(0, n - 1)], r.xs.at[0])
    left(r.cbuf.at[pl.ds(0, n - 1)], r.cs.at[0])
    left(r.abuf.at[pl.ds(0, n - 1)], r.as_.at[0])
    left(r.bbuf.at[pl.ds(0, n - 1)], r.bs.at[0])
    left(r.sbuf1.at[0, pl.ds(0, n - 1)], r.s1s.at[0])
    left(r.sbuf2.at[0, pl.ds(0, n - 1)], r.s2s.at[0])
    left(r.resid.at[0, pl.ds(0, n - 1)], r.fs.at[0])
    if half > 1:
        left(r.resid.at[pl.ds(0, half - 1)], r.gs.at[0])
    left(r.wide_ow.at[pl.ds(0, (m - 1) * vc)], r.ows.at[0])
    for c in e_copies + s_copies:
        c.wait_send()

    @pl.when(at_home)
    def _():
        left(r.tsend.at[pl.ds(0, n - 1)], r.ts.at[0])
        left(r.hbuf.at[pl.ds(0, n - 1)], r.hs.at[0])

    @pl.when(jnp.logical_not(at_home))
    def _():
        left(r.hbuf, r.hs.at[0])

    @pl.when(held_here)
    def _():
        arrived(r.rbuf.at[pl.ds(0, n * half - 1)], r.rr.at[0])

    @pl.when(jnp.logical_not(held_here))
    def _():
        arrived(r.rbuf, r.rr.at[0])
        arrived(r.rown, r.dr.at[0])

    acc = jnp.concatenate([r.rown[b].astype(F32) for b in range(group)], axis=1)
    for p in range(n * half):
        acc = acc + r.rbuf[p].astype(F32)
    r.obuf[tp] = acc.astype(BF16)
    for i in range(1, m):
        t = lax.rem(tp + i, m)
        remote(r.obuf.at[tp], r.obuf.at[tp], r.os_.at[0], r.or_.at[0], me, t).start()

    @pl.when(held_here)
    def _():
        d_copy.wait_send()
        left(r.rbuf.at[pl.ds(0, n * half - 1)], r.rs.at[0])

    @pl.when(jnp.logical_not(held_here))
    def _():
        left(r.rbuf, r.rs.at[0])

    arrived(r.obuf.at[pl.ds(0, m - 1)], r.or_.at[0])
    for t in range(m):
        r.out[:, t * quarter : (t + 1) * quarter] = r.obuf[t]
    left(r.obuf.at[pl.ds(0, m - 1)], r.os_.at[0])


def flush_kernel(layer_ref, state_ref, layer_out, state_out, sem):
    rows = state_ref.shape[0]
    part = rows // STATE_PARTS
    copies = [pltpu.make_async_copy(layer_ref, layer_out, sem.at[STATE_PARTS])]
    for i in range(STATE_PARTS):
        these = pl.ds(i * part, part)
        copies.append(
            pltpu.make_async_copy(state_ref.at[these], state_out.at[these], sem.at[i])
        )
    for c in copies:
        c.start()
    for c in copies:
        c.wait()


VMEM = pl.BlockSpec(memory_space=pltpu.VMEM)
HBM = pl.BlockSpec(memory_space=pltpu.HBM)


def per_device(
    n,
    m,
    tokens,
    norm_gain,
    query_weight,
    key_weight,
    value_weight,
    outgate_weight,
    beta_weight,
    decay_weight,
    decay_rate,
    decay_bias,
    head_gain,
    recurrent,
    output_weight,
    ffn_gain,
    routes,
    route_weight,
    expert_gate,
    expert_up,
    expert_down,
    shared_gate,
    shared_up,
    shared_down,
    branch_gate,
):
    rows, width = tokens.shape
    _, heads, key_dim, value_dim = recurrent.shape
    depth, qc = query_weight.shape
    vc = value_weight.shape[1]
    keys = qc // key_dim
    near = 2 * qc + vc
    half = m // 2
    group = n // m
    units = shared_gate.shape[1] // n
    cols = shared_down.shape[1]
    hidden = expert_gate.shape[2]
    quarter = width // m
    sds = jax.ShapeDtypeStruct
    dma = pltpu.SemaphoreType.DMA

    inputs = dict(
        tokens=tokens,
        gain=norm_gain,
        qw=query_weight,
        kw=key_weight,
        vw=value_weight,
        gw=outgate_weight,
        beta=beta_weight.T,
        decay=decay_weight.T,
        rate=decay_rate[None, :],
        bias=decay_bias[None, :],
        routes=routes.T,
        rw=route_weight.T,
        head_gain=head_gain,
        state=recurrent,
        ow=output_weight,
        ffn_gain=ffn_gain,
        eg=expert_gate,
        eu=expert_up,
        ed=expert_down,
        sg=shared_gate,
        su=shared_up,
        sd=shared_down,
        bg=branch_gate,
    )
    plain = ("tokens", "gain", "beta", "decay", "rate", "bias", "routes", "rw")
    plain += ("head_gain", "ffn_gain", "sg", "su", "sd", "bg")
    scratch = {k: pltpu.VMEM(inputs[k].shape, inputs[k].dtype) for k in plain}
    scratch.update(
        weights=pltpu.VMEM((depth, near + vc), BF16),
        wide_ow=pltpu.VMEM((m * vc, cols), BF16),
        eg=pltpu.VMEM((width, 2 * hidden), BF16),
        eu=pltpu.VMEM((width, 2 * hidden), BF16),
        ed=pltpu.VMEM((2 * hidden, width), BF16),
        xsend=pltpu.VMEM((n, rows, depth), BF16),
        xbuf=pltpu.VMEM((n, rows, depth), BF16),
        csend=pltpu.VMEM((n, rows, 128), BF16),
        cbuf=pltpu.VMEM((n, rows, 128), BF16),
        tsend=pltpu.VMEM((n, rows, depth), BF16),
        tbuf=pltpu.VMEM((group, rows, depth), BF16),
        ssend1=pltpu.VMEM((n, 2 * units, cols), BF16),
        sbuf1=pltpu.VMEM((2, n, 2 * units, cols), BF16),
        ssend2=pltpu.VMEM((n, units, cols), BF16),
        sbuf2=pltpu.VMEM((2, n, units, cols), BF16),
        shared=pltpu.VMEM((2, 3 * units, width), BF16),
        asend=pltpu.VMEM((n, rows, near), BF16),
        abuf=pltpu.VMEM((n, rows, near), BF16),
        bsend=pltpu.VMEM((n, rows, vc), BF16),
        bbuf=pltpu.VMEM((n, rows, vc), BF16),
        retain=pltpu.VMEM((rows, vc), F32),
        pull=pltpu.VMEM((rows, vc), F32),
        push=pltpu.VMEM((rows, vc), F32),
        qk=pltpu.VMEM((rows, keys * value_dim), F32),
        kq=pltpu.VMEM((key_dim, 128), F32),
        held=pltpu.VMEM((rows, vc), F32),
        routed=pltpu.VMEM((half, group * rows, 128), F32),
        hsend=pltpu.VMEM((rows, vc), BF16),
        hbuf=pltpu.VMEM((n, rows, vc), BF16),
        resid=pltpu.VMEM((half, n, group, rows, cols), BF16),
        rown=pltpu.VMEM((group, rows, cols), BF16),
        rsend=pltpu.VMEM((half, group, m, rows, quarter), BF16),
        rbuf=pltpu.VMEM((n * half, rows, quarter), BF16),
        obuf=pltpu.VMEM((m, rows, quarter), BF16),
        wsem=dma((len(inputs) - 5,)),
        psem=dma((2,)),
    )
    counts = dict(xr=4, fr=n, gr=half, es=3, er=3, ps=2, pr=2)
    for name in ("x", "c", "ow", "a", "b", "t", "s1", "s2", "h", "f", "g", "e", "p", "d", "r", "o"):
        for end in ("s", "r"):
            key = {"as": "as_", "os": "os_", "or": "or_"}.get(name + end, name + end)
            scratch[key] = dma((counts.get(key, 1),))
    names = [k + "_hbm" for k in inputs] + ["out", "new"] + list(scratch)
    layer, state = pl.pallas_call(
        functools.partial(layer_kernel, n, m, names),
        out_shape=(pltpu.VMEM((rows, width), BF16), pltpu.VMEM(recurrent.shape, F32)),
        in_specs=[HBM] * len(inputs),
        out_specs=(VMEM, VMEM),
        scratch_shapes=list(scratch.values()),
        compiler_params=pltpu.CompilerParams(
            collective_id=0, has_side_effects=True, vmem_limit_bytes=48 * 2**20
        ),
    )(*(pltpu.with_memory_space_constraint(v, pltpu.HBM) for v in inputs.values()))

    return pl.pallas_call(
        flush_kernel,
        out_shape=(sds((rows, width), BF16), sds(recurrent.shape, F32)),
        in_specs=[VMEM, VMEM],
        out_specs=(HBM, HBM),
        scratch_shapes=[dma((STATE_PARTS + 1,))],
        compiler_params=pltpu.CompilerParams(vmem_limit_bytes=4 * 2**20),
    )(layer, state)


def solution(mesh):
    return jax.shard_map(
        functools.partial(per_device, mesh.shape["ep"], mesh.shape["tp"]),
        mesh=mesh,
        in_specs=(
            P("ep", None),
            P(),
            P("ep", "tp"),
            P("ep", "tp"),
            P("ep", "tp"),
            P("ep", "tp"),
            P(),
            P(),
            P("tp"),
            P("tp"),
            P(),
            P("ep", "tp", None, None),
            P("tp", "ep"),
            P(),
            P("ep", None),
            P("ep", None),
            P("ep", None, "tp"),
            P("ep", None, "tp"),
            P("ep", "tp", None),
            P("ep", "tp"),
            P("ep", "tp"),
            P("tp", "ep"),
            P(),
        ),
        out_specs=(P("ep", None), P("ep", "tp", None, None)),
        check_vma=False,
    )
```

```python
import functools
import types

import jax
import jax.numpy as jnp
from jax import lax
from jax.experimental import pallas as pl
from jax.experimental.pallas import tpu as pltpu
from jax.sharding import PartitionSpec as P

EPS = 1e-06
ROUTED_SCALE = 2.5
MESH = pl.DeviceIdType.MESH
F32 = jnp.float32
BF16 = jnp.bfloat16
STATE_PARTS = 4


def silu(v):
    return v / (1.0 + jnp.exp(-v))


def sigmoid(v):
    return 1.0 / (1.0 + jnp.exp(-v))


def rms_scale(values, gain):
    values = values.astype(F32)
    return (
        values
        * lax.rsqrt(jnp.mean(values * values, axis=-1, keepdims=True) + EPS)
        * gain.astype(F32).reshape(1, -1)
    )


def unit_rows(values):
    return values * lax.rsqrt(jnp.sum(values * values, axis=-1, keepdims=True) + EPS)


def dot(a, b):
    return jnp.dot(a, b, preferred_element_type=F32)


def dot_nt(a, b):
    return lax.dot_general(a, b, (((1,), (1,)), ((), ())), preferred_element_type=F32)


def remote(src, dst, send_sem, recv_sem, e, t):
    return pltpu.make_async_remote_copy(
        src_ref=src,
        dst_ref=dst,
        send_sem=send_sem,
        recv_sem=recv_sem,
        device_id=(e, t),
        device_id_type=MESH,
    )


def loop(lo, hi, body):
    def step(i, c):
        body(i)
        return c

    lax.fori_loop(lo, hi, step, 0)


def layer_kernel(n, m, names, *refs):
    r = types.SimpleNamespace(**dict(zip(names, refs)))
    me, tp = lax.axis_index("ep"), lax.axis_index("tp")
    half = m // 2
    group = n // m
    core = lax.rem(tp, 2)
    pair = tp + 1 - 2 * core
    xi = tp // 2
    home = lax.rem(me, m)
    turn = me // m
    rows, width = r.tokens.shape
    depth, qc = r.qw_hbm.shape
    vc = r.vw_hbm.shape[1]
    key_dim, value_dim = r.new.shape[2], r.new.shape[3]
    heads = r.new.shape[1]
    keys = qc // key_dim
    share = heads // keys
    near = 2 * qc + vc
    cols = r.wide_ow.shape[1]
    hidden = r.eg_hbm.shape[2]
    quarter = width // m
    units = r.ssend2.shape[1]
    tall = group * rows

    barrier = pltpu.get_barrier_semaphore()

    steps = [
        (1 - 2 * lax.rem(me // 2**i, 2)) * 2**i for i in range(n.bit_length() - 1)
    ]

    def peer(k):
        p = me
        for i, step in enumerate(steps):
            if k >> i & 1:
                p = p + step
        return p

    cuts = (n // 2, 3 * n // 4, n), (n // 4, n // 2), (0, n // 4)
    spans = [cuts[0][:2], cuts[0][1:], cuts[1], cuts[2]]
    order = [k for lo, hi in spans for k in range(lo, hi) if k]

    for k in order:
        pl.semaphore_signal(barrier, inc=1, device_id=(peer(k), tp), device_id_type=MESH)
    for i in range(1, m):
        pl.semaphore_signal(
            barrier, inc=1, device_id=(me, lax.rem(tp + i, m)), device_id_type=MESH
        )

    fetches, alone = {}, []

    def fetch(name, src, dst, sem=None):
        if sem is None:
            sem = r.wsem.at[len(alone)]
            alone.append(name)
        c = pltpu.make_async_copy(src, dst, sem)
        c.start()
        fetches[name] = c

    for name in ("tokens", "gain"):
        fetch(name, getattr(r, name + "_hbm"), getattr(r, name))
    at = 0
    for name in ("qw", "kw", "vw", "gw"):
        src = getattr(r, name + "_hbm")
        fetch(name, src, r.weights.at[:, pl.ds(at, src.shape[1])], r.psem.at[0])
        at += src.shape[1]
    for name in ("routes", "rw", "sd", "beta", "decay", "rate", "bias", "sg", "su"):
        fetch(name, getattr(r, name + "_hbm"), getattr(r, name))
    part = rows // STATE_PARTS
    for i in range(STATE_PARTS):
        these = pl.ds(i * part, part)
        fetch(("state", i), r.state_hbm.at[these], r.new.at[these], r.psem.at[1])
    for name in ("head_gain", "ffn_gain", "bg"):
        fetch(name, getattr(r, name + "_hbm"), getattr(r, name))
    own_ow = pl.ds(pl.multiple_of(tp * vc, vc), vc)
    mine = pl.ds(pl.multiple_of(core * hidden, hidden), hidden)
    other = pl.ds(pl.multiple_of((1 - core) * hidden, hidden), hidden)
    fetch("ow", r.ow_hbm, r.wide_ow.at[own_ow])
    fetch("eg", r.eg_hbm.at[0], r.eg.at[:, mine])
    fetch("eu", r.eu_hbm.at[0], r.eu.at[:, mine])
    fetch("ed", r.ed_hbm.at[0], r.ed.at[mine])

    def arrived(ref, sem):
        remote(ref, ref, sem, sem, me, pair).wait_recv()

    def left(ref, sem):
        remote(ref, ref, sem, sem, me, pair).wait_send()

    fetches["tokens"].wait()
    fetches["gain"].wait()
    tokens = r.tokens[...]
    normed = rms_scale(tokens, r.gain[...]).astype(BF16)
    for e in range(n):
        r.xsend[e] = normed[:, e * depth : (e + 1) * depth]
        r.tsend[e] = tokens[:, e * depth : (e + 1) * depth]

    fetches["routes"].wait()
    fetches["rw"].wait()
    rw = r.rw[...]
    scaled = rw / jnp.sum(rw, axis=0, keepdims=True) * ROUTED_SCALE
    routes = r.routes[...]
    expert = lax.broadcasted_iota(jnp.int32, (128, rows), 0)
    by_expert = jnp.zeros((128, rows), F32)
    for k in range(routes.shape[0]):
        by_expert = by_expert + jnp.where(
            expert == routes[k : k + 1, :], scaled[k : k + 1, :], 0.0
        )
    by_expert = by_expert.T
    lane = lax.broadcasted_iota(jnp.int32, (rows, 128), 1)
    for e in range(n):
        w = by_expert[:, e : e + 1]
        high = w.astype(BF16).astype(F32)
        r.csend[e] = jnp.where(lane < 64, high, w - high).astype(BF16)
    fetches["sd"].wait()
    for e in range(n):
        r.ssend2[e] = r.sd[e * units : (e + 1) * units]
    pl.semaphore_wait(barrier, n + m - 2)

    for g, (lo, hi) in enumerate(spans):
        for k in range(max(lo, 1), hi):
            p = peer(k)
            remote(r.xsend.at[p], r.xbuf.at[k], r.xs.at[0], r.xr.at[g], p, tp).start()
    r.xbuf[0] = r.xsend[me]
    for k in order:
        p = peer(k)
        remote(r.csend.at[p], r.cbuf.at[me], r.cs.at[0], r.cr.at[0], p, tp).start()
    r.cbuf[me] = r.csend[me]

    def send_shared(src, dst, s, d):
        for k in order:
            p = peer(k)
            remote(src.at[p], dst.at[core, me], s.at[0], d.at[0], p, tp).start()
        dst[core, me] = src[me]

    send_shared(r.ssend2, r.sbuf2, r.s2s, r.s2r)

    for i in range(1, m):
        t = lax.rem(tp + i, m)
        remote(r.ow_hbm, r.wide_ow.at[own_ow], r.ows.at[0], r.owr.at[0], me, t).start()
    e_copies = [
        remote(r.eg_hbm.at[0], r.eg.at[:, mine], r.es.at[0], r.er.at[0], me, pair),
        remote(r.eu_hbm.at[0], r.eu.at[:, mine], r.es.at[1], r.er.at[1], me, pair),
        remote(r.ed_hbm.at[0], r.ed.at[mine], r.es.at[2], r.er.at[2], me, pair),
    ]
    for c in e_copies:
        c.start()

    for name in ("beta", "decay", "rate", "bias", "sg", "su"):
        fetches[name].wait()
    column = lax.broadcasted_iota(jnp.int32, (rows, r.beta.shape[0]), 1)

    def own_heads(w):
        logits = dot_nt(normed, w)
        return [
            jnp.sum(jnp.where(column == tp * heads + h, logits, 0.0), axis=1, keepdims=True)
            for h in range(heads)
        ]

    def wide(v):
        return jnp.broadcast_to(v, (rows, value_dim))

    beta = own_heads(r.beta[...])
    decay = own_heads(r.decay[...])
    for h in range(heads):
        at = slice(h * value_dim, (h + 1) * value_dim)
        strength = sigmoid(wide(beta[h]))
        shifted = wide(decay[h]) + r.bias[:, h : h + 1]
        softplus = jnp.maximum(shifted, 0.0) + jnp.log1p(jnp.exp(-jnp.abs(shifted)))
        retain = jnp.exp(-r.rate[:, h : h + 1] * softplus)
        r.retain[:, at] = retain
        r.pull[:, at] = strength * retain
        r.push[:, at] = strength
    for at, name in enumerate(("sg", "su")):
        by_unit = getattr(r, name)[...].astype(F32).T.astype(BF16)
        for e in range(n):
            r.ssend1[e, at * units : (at + 1) * units] = by_unit[e * units : (e + 1) * units]

    pltpu.make_async_copy(r.weights, r.weights, r.psem.at[0]).wait()
    for g, (lo, hi) in enumerate(spans):
        if hi > max(lo, 1):
            arrived(r.xbuf.at[pl.ds(max(lo, 1), hi - max(lo, 1))], r.xr.at[g])
        x = r.xbuf[lo:hi].reshape((hi - lo) * rows, depth)
        for c in range(0, near, 512):
            size = min(512, near - c)
            out = dot(x, r.weights[:, c : c + size])
            r.asend[lo:hi, :, c : c + size] = out.astype(BF16).reshape(hi - lo, rows, size)
        for k in range(max(lo, 1), hi):
            remote(
                r.asend.at[k], r.abuf.at[k], r.as_.at[0], r.ar.at[0], peer(k), tp
            ).start()
    r.abuf[0] = r.asend[0]
    x = r.xbuf[...].reshape(n * rows, depth)
    out = dot(x, r.weights[:, near:])
    r.bsend[...] = out.astype(BF16).reshape(n, rows, vc)
    for k in order:
        remote(r.bsend.at[k], r.bbuf.at[k], r.bs.at[0], r.br.at[0], peer(k), tp).start()
    r.bbuf[0] = r.bsend[0]

    at_home = tp == home

    @pl.when(at_home)
    def _():
        for k in order:
            p = peer(k)
            remote(
                r.tsend.at[p], r.tbuf.at[turn], r.ts.at[0], r.tr.at[0], p, tp
            ).start()
        r.tbuf[turn] = r.tsend[me]

    arrived(r.cbuf.at[pl.ds(0, n - 1)], r.cr.at[0])
    for a in range(half):
        for b in range(group):
            w = r.cbuf[b * m + 2 * a + core].astype(F32)
            r.routed[a, b * rows : (b + 1) * rows] = jnp.broadcast_to(
                w[:, 0:1] + w[:, 64:65], (rows, 128)
            )
    fetches["head_gain"].wait()
    pltpu.make_async_copy(r.new, r.new, r.psem.at[1]).wait()

    arrived(r.abuf.at[pl.ds(1, n - 1)], r.ar.at[0])

    def gathered(ref, c, size):
        acc = ref[0, :, c : c + size].astype(F32)
        for e in range(1, n):
            acc = acc + ref[e, :, c : c + size].astype(F32)
        return acc.astype(BF16).astype(F32)

    q_rows = [
        unit_rows(silu(gathered(r.abuf, j * key_dim, key_dim))) * key_dim ** (-0.5)
        for j in range(keys)
    ]
    k_rows = [
        unit_rows(silu(gathered(r.abuf, qc + j * key_dim, key_dim))) for j in range(keys)
    ]
    for h in range(heads):
        at = slice(h * value_dim, (h + 1) * value_dim)
        r.push[:, at] = r.push[:, at] * silu(
            gathered(r.abuf, 2 * qc + h * value_dim, value_dim)
        )
    for j in range(keys):
        r.qk[:, j * value_dim : (j + 1) * value_dim] = wide(
            jnp.sum(q_rows[j] * k_rows[j], axis=1, keepdims=True)
        )
    stacked = q_rows + k_rows
    stacked.append(jnp.zeros((128 - 2 * keys * rows, key_dim), F32))
    r.kq[...] = jnp.concatenate(stacked, axis=0).T

    for j in range(keys):
        for s in range(rows):
            q = jnp.broadcast_to(r.kq[:, j * rows + s : j * rows + s + 1], (key_dim, value_dim))
            at = (keys + j) * rows + s
            k = jnp.broadcast_to(r.kq[:, at : at + 1], (key_dim, value_dim))
            one = slice(s, s + 1)
            qk = r.qk[one, j * value_dim : (j + 1) * value_dim]
            for h in range(j * share, (j + 1) * share):
                c = slice(h * value_dim, (h + 1) * value_dim)
                state = r.new[s, h]
                retain = r.retain[one, c]
                predicted = jnp.sum(state * k, axis=0, keepdims=True)
                before = jnp.sum(state * q, axis=0, keepdims=True)
                correction = r.push[one, c] - r.pull[one, c] * predicted
                r.new[s, h] = state * retain + k * correction
                r.held[one, c] = before * retain + qk * correction

    arrived(r.bbuf.at[pl.ds(1, n - 1)], r.br.at[0])
    for h in range(heads):
        c = slice(h * value_dim, (h + 1) * value_dim)
        gate = silu(gathered(r.bbuf, h * value_dim, value_dim))
        r.hsend[:, c] = (rms_scale(r.held[:, c], r.head_gain[...]) * gate).astype(BF16)

    def send_h(p):
        remote(
            r.hsend, r.hbuf.at[turn * m + tp], r.hs.at[0], r.hr.at[0], p, home
        ).start()

    for k in order:
        send_h(peer(k))

    @pl.when(jnp.logical_not(at_home))
    def _():
        send_h(me)

    @pl.when(at_home)
    def _():
        r.hbuf[turn * m + tp] = r.hsend[...]

    send_shared(r.ssend1, r.sbuf1, r.s1s, r.s1r)

    fetches["ow"].wait()
    arrived(r.wide_ow.at[pl.ds(0, (m - 1) * vc)], r.owr.at[0])

    @pl.when(at_home)
    def _():
        arrived(r.tbuf.at[pl.ds(0, group - 1)], r.tr.at[0])
        arrived(r.hbuf.at[pl.ds(0, n - 1)], r.hr.at[0])

    @pl.when(jnp.logical_not(at_home))
    def _():
        arrived(r.tbuf, r.tr.at[0])
        arrived(r.hbuf, r.hr.at[0])

    residual = r.tbuf[...].reshape(tall, cols).astype(F32)
    mix = None
    for t in range(m):
        h = jnp.concatenate([r.hbuf[b * m + t] for b in range(group)], axis=0)
        term = dot(h, r.wide_ow[t * vc : (t + 1) * vc])
        mix = term if mix is None else mix + term
    r.resid[xi, me] = (residual + mix).astype(BF16).reshape(group, rows, cols)

    mine_resid = r.resid.at[xi, me]
    for k in order:
        remote(mine_resid, mine_resid, r.fs.at[0], r.fr.at[k], peer(k), tp).start()

    def f_pass(p):
        ref = r.resid.at[xi, p]
        for i in range(1, half):
            t = 2 * lax.rem(xi + i, half) + core
            remote(ref, ref, r.gs.at[0], r.gr.at[xi], me, t).start()

    f_pass(me)
    arrived(r.sbuf1.at[0, pl.ds(0, n - 1)], r.s1r.at[0])
    s_copies = [remote(r.sbuf1.at[core], r.sbuf1.at[core], r.ps.at[0], r.pr.at[0], me, pair)]
    s_copies[0].start()
    arrived(r.sbuf2.at[0, pl.ds(0, n - 1)], r.s2r.at[0])
    s_copies.append(
        remote(r.sbuf2.at[core], r.sbuf2.at[core], r.ps.at[1], r.pr.at[1], me, pair)
    )
    s_copies[1].start()
    for k in reversed(order):
        p = peer(k)
        arrived(r.resid.at[xi, p], r.fr.at[k])
        f_pass(p)
    arrived(r.sbuf1.at[0], r.pr.at[0])
    arrived(r.sbuf2.at[0], r.pr.at[1])
    for c in range(2):
        r.shared[c, : 2 * units] = jnp.concatenate([r.sbuf1[c, e] for e in range(n)], axis=1)
        r.shared[c, 2 * units :] = jnp.concatenate([r.sbuf2[c, e] for e in range(n)], axis=1)
    for name in ("ffn_gain", "bg", "eg", "eu", "ed"):
        fetches[name].wait()
    for i, ref in enumerate((r.eg.at[:, other], r.eu.at[:, other], r.ed.at[other])):
        arrived(ref, r.er.at[i])

    gain = r.ffn_gain[...].astype(F32).reshape(1, -1)
    bg = r.bg[...].astype(F32).reshape(1, -1)
    upper = me // (n // 2)

    def target(a, b):
        return b * m + 2 * a + core

    def away(a, b, q):
        return jnp.logical_or(target(a, b) != me, q != tp)

    def work(a):
        blocks = [r.resid[a, e].reshape(tall, cols).astype(F32) for e in range(n)]
        square = blocks[0] * blocks[0]
        for v in blocks[1:]:
            square = square + v * v
        scale = lax.rsqrt(jnp.sum(square, axis=1, keepdims=True) / width + EPS)
        ffn = jnp.concatenate(
            [
                (v * scale * gain[:, e * cols : (e + 1) * cols]).astype(BF16)
                for e, v in enumerate(blocks)
            ],
            axis=1,
        )
        act = (silu(dot(ffn, r.eg[...])) * dot(ffn, r.eu[...])).astype(BF16)
        dense = []
        for c in range(2):
            both = dot_nt(ffn, r.shared[c, : 2 * units])
            dense.append((silu(both[:, :units]) * both[:, units:]).astype(BF16))
        branch = sigmoid(jnp.sum(ffn.astype(F32) * bg, axis=1, keepdims=True))
        weight = r.routed[a, :, 0:1]
        for k in range(m):
            q = lax.rem(tp + k, m)
            at = pl.ds(pl.multiple_of(q * quarter, quarter), quarter)
            out = weight * dot(act, r.ed[:, at])
            side = dot(dense[0], r.shared[0, 2 * units :, at])
            side = side + dot(dense[1], r.shared[1, 2 * units :, at])
            r.rsend[a, :, q] = (out + branch * side).astype(BF16).reshape(group, rows, quarter)
            for i in range(group):
                b = lax.rem(i + (group // 2) * (1 - upper), group)

                @pl.when(away(a, b, q))
                def _():
                    remote(
                        r.rsend.at[a, b, q],
                        r.rbuf.at[me * half + xi],
                        r.rs.at[0],
                        r.rr.at[0],
                        target(a, b),
                        q,
                    ).start()

    work(xi)
    for i in range(1, half):
        a = lax.rem(xi + i, half)
        arrived(r.resid.at[a], r.gr.at[a])
        work(a)

    held_here = core == lax.rem(home, 2)
    place = home // 2
    d_copy = remote(
        r.resid.at[place, pl.ds(pair * group, group), turn],
        r.rown,
        r.ds.at[0],
        r.dr.at[0],
        me,
        pair,
    )

    @pl.when(held_here)
    def _():
        d_copy.start()
        r.rown[...] = r.resid[place, pl.ds(tp * group, group), turn]
        r.rbuf[me * half + xi] = r.rsend[place, turn, tp]

    left(r.xbuf.at[pl.ds(0, n - 1)], r.xs.at[0])
    left(r.cbuf.at[pl.ds(0, n - 1)], r.cs.at[0])
    left(r.abuf.at[pl.ds(0, n - 1)], r.as_.at[0])
    left(r.bbuf.at[pl.ds(0, n - 1)], r.bs.at[0])
    left(r.sbuf1.at[0, pl.ds(0, n - 1)], r.s1s.at[0])
    left(r.sbuf2.at[0, pl.ds(0, n - 1)], r.s2s.at[0])
    left(r.resid.at[0, pl.ds(0, n - 1)], r.fs.at[0])
    if half > 1:
        left(r.resid.at[pl.ds(0, half - 1)], r.gs.at[0])
    left(r.wide_ow.at[pl.ds(0, (m - 1) * vc)], r.ows.at[0])
    for c in e_copies + s_copies:
        c.wait_send()

    @pl.when(at_home)
    def _():
        left(r.tsend.at[pl.ds(0, n - 1)], r.ts.at[0])
        left(r.hbuf.at[pl.ds(0, n - 1)], r.hs.at[0])

    @pl.when(jnp.logical_not(at_home))
    def _():
        left(r.hbuf, r.hs.at[0])

    @pl.when(held_here)
    def _():
        arrived(r.rbuf.at[pl.ds(0, n * half - 1)], r.rr.at[0])

    @pl.when(jnp.logical_not(held_here))
    def _():
        arrived(r.rbuf, r.rr.at[0])
        arrived(r.rown, r.dr.at[0])

    acc = jnp.concatenate([r.rown[b].astype(F32) for b in range(group)], axis=1)
    for p in range(n * half):
        acc = acc + r.rbuf[p].astype(F32)
    r.obuf[tp] = acc.astype(BF16)
    for i in range(1, m):
        t = lax.rem(tp + i, m)
        remote(r.obuf.at[tp], r.obuf.at[tp], r.os_.at[0], r.or_.at[0], me, t).start()

    @pl.when(held_here)
    def _():
        d_copy.wait_send()
        left(r.rbuf.at[pl.ds(0, n * half - 1)], r.rs.at[0])

    @pl.when(jnp.logical_not(held_here))
    def _():
        left(r.rbuf, r.rs.at[0])

    arrived(r.obuf.at[pl.ds(0, m - 1)], r.or_.at[0])
    for t in range(m):
        r.out[:, t * quarter : (t + 1) * quarter] = r.obuf[t]
    left(r.obuf.at[pl.ds(0, m - 1)], r.os_.at[0])


def flush_kernel(layer_ref, state_ref, layer_out, state_out, sem):
    rows = state_ref.shape[0]
    part = rows // STATE_PARTS
    copies = [pltpu.make_async_copy(layer_ref, layer_out, sem.at[STATE_PARTS])]
    for i in range(STATE_PARTS):
        these = pl.ds(i * part, part)
        copies.append(
            pltpu.make_async_copy(state_ref.at[these], state_out.at[these], sem.at[i])
        )
    for c in copies:
        c.start()
    for c in copies:
        c.wait()


VMEM = pl.BlockSpec(memory_space=pltpu.VMEM)
HBM = pl.BlockSpec(memory_space=pltpu.HBM)


def per_device(
    n,
    m,
    tokens,
    norm_gain,
    query_weight,
    key_weight,
    value_weight,
    outgate_weight,
    beta_weight,
    decay_weight,
    decay_rate,
    decay_bias,
    head_gain,
    recurrent,
    output_weight,
    ffn_gain,
    routes,
    route_weight,
    expert_gate,
    expert_up,
    expert_down,
    shared_gate,
    shared_up,
    shared_down,
    branch_gate,
):
    rows, width = tokens.shape
    _, heads, key_dim, value_dim = recurrent.shape
    depth, qc = query_weight.shape
    vc = value_weight.shape[1]
    keys = qc // key_dim
    near = 2 * qc + vc
    half = m // 2
    group = n // m
    units = shared_gate.shape[1] // n
    cols = shared_down.shape[1]
    hidden = expert_gate.shape[2]
    quarter = width // m
    sds = jax.ShapeDtypeStruct
    dma = pltpu.SemaphoreType.DMA

    inputs = dict(
        tokens=tokens,
        gain=norm_gain,
        qw=query_weight,
        kw=key_weight,
        vw=value_weight,
        gw=outgate_weight,
        beta=beta_weight.T,
        decay=decay_weight.T,
        rate=decay_rate[None, :],
        bias=decay_bias[None, :],
        routes=routes.T,
        rw=route_weight.T,
        head_gain=head_gain,
        state=recurrent,
        ow=output_weight,
        ffn_gain=ffn_gain,
        eg=expert_gate,
        eu=expert_up,
        ed=expert_down,
        sg=shared_gate,
        su=shared_up,
        sd=shared_down,
        bg=branch_gate,
    )
    plain = ("tokens", "gain", "beta", "decay", "rate", "bias", "routes", "rw")
    plain += ("head_gain", "ffn_gain", "sg", "su", "sd", "bg")
    scratch = {k: pltpu.VMEM(inputs[k].shape, inputs[k].dtype) for k in plain}
    scratch.update(
        weights=pltpu.VMEM((depth, near + vc), BF16),
        wide_ow=pltpu.VMEM((m * vc, cols), BF16),
        eg=pltpu.VMEM((width, 2 * hidden), BF16),
        eu=pltpu.VMEM((width, 2 * hidden), BF16),
        ed=pltpu.VMEM((2 * hidden, width), BF16),
        xsend=pltpu.VMEM((n, rows, depth), BF16),
        xbuf=pltpu.VMEM((n, rows, depth), BF16),
        csend=pltpu.VMEM((n, rows, 128), BF16),
        cbuf=pltpu.VMEM((n, rows, 128), BF16),
        tsend=pltpu.VMEM((n, rows, depth), BF16),
        tbuf=pltpu.VMEM((group, rows, depth), BF16),
        ssend1=pltpu.VMEM((n, 2 * units, cols), BF16),
        sbuf1=pltpu.VMEM((2, n, 2 * units, cols), BF16),
        ssend2=pltpu.VMEM((n, units, cols), BF16),
        sbuf2=pltpu.VMEM((2, n, units, cols), BF16),
        shared=pltpu.VMEM((2, 3 * units, width), BF16),
        asend=pltpu.VMEM((n, rows, near), BF16),
        abuf=pltpu.VMEM((n, rows, near), BF16),
        bsend=pltpu.VMEM((n, rows, vc), BF16),
        bbuf=pltpu.VMEM((n, rows, vc), BF16),
        retain=pltpu.VMEM((rows, vc), F32),
        pull=pltpu.VMEM((rows, vc), F32),
        push=pltpu.VMEM((rows, vc), F32),
        qk=pltpu.VMEM((rows, keys * value_dim), F32),
        kq=pltpu.VMEM((key_dim, 128), F32),
        held=pltpu.VMEM((rows, vc), F32),
        routed=pltpu.VMEM((half, group * rows, 128), F32),
        hsend=pltpu.VMEM((rows, vc), BF16),
        hbuf=pltpu.VMEM((n, rows, vc), BF16),
        resid=pltpu.VMEM((half, n, group, rows, cols), BF16),
        rown=pltpu.VMEM((group, rows, cols), BF16),
        rsend=pltpu.VMEM((half, group, m, rows, quarter), BF16),
        rbuf=pltpu.VMEM((n * half, rows, quarter), BF16),
        obuf=pltpu.VMEM((m, rows, quarter), BF16),
        wsem=dma((len(inputs) - 5,)),
        psem=dma((2,)),
    )
    counts = dict(xr=4, fr=n, gr=half, es=3, er=3, ps=2, pr=2)
    for name in ("x", "c", "ow", "a", "b", "t", "s1", "s2", "h", "f", "g", "e", "p", "d", "r", "o"):
        for end in ("s", "r"):
            key = {"as": "as_", "os": "os_", "or": "or_"}.get(name + end, name + end)
            scratch[key] = dma((counts.get(key, 1),))
    names = [k + "_hbm" for k in inputs] + ["out", "new"] + list(scratch)
    layer, state = pl.pallas_call(
        functools.partial(layer_kernel, n, m, names),
        out_shape=(pltpu.VMEM((rows, width), BF16), pltpu.VMEM(recurrent.shape, F32)),
        in_specs=[HBM] * len(inputs),
        out_specs=(VMEM, VMEM),
        scratch_shapes=list(scratch.values()),
        compiler_params=pltpu.CompilerParams(
            collective_id=0, has_side_effects=True, vmem_limit_bytes=48 * 2**20
        ),
    )(*(pltpu.with_memory_space_constraint(v, pltpu.HBM) for v in inputs.values()))

    return pl.pallas_call(
        flush_kernel,
        out_shape=(sds((rows, width), BF16), sds(recurrent.shape, F32)),
        in_specs=[VMEM, VMEM],
        out_specs=(HBM, HBM),
        scratch_shapes=[dma((STATE_PARTS + 1,))],
        compiler_params=pltpu.CompilerParams(vmem_limit_bytes=4 * 2**20),
    )(layer, state)


def solution(mesh):
    return jax.shard_map(
        functools.partial(per_device, mesh.shape["ep"], mesh.shape["tp"]),
        mesh=mesh,
        in_specs=(
            P("ep", None),
            P(),
            P("ep", "tp"),
            P("ep", "tp"),
            P("ep", "tp"),
            P("ep", "tp"),
            P(),
            P(),
            P("tp"),
            P("tp"),
            P(),
            P("ep", "tp", None, None),
            P("tp", "ep"),
            P(),
            P("ep", None),
            P("ep", None),
            P("ep", None, "tp"),
            P("ep", None, "tp"),
            P("ep", "tp", None),
            P("ep", "tp"),
            P("ep", "tp"),
            P("tp", "ep"),
            P(),
        ),
        out_specs=(P("ep", None), P("ep", "tp", None, None)),
        check_vma=False,
    )
```

```python
import functools
import types

import jax
import jax.numpy as jnp
from jax import lax
from jax.experimental import pallas as pl
from jax.experimental.pallas import tpu as pltpu
from jax.sharding import PartitionSpec as P

EPS = 1e-06
ROUTED_SCALE = 2.5
MESH = pl.DeviceIdType.MESH
F32 = jnp.float32
BF16 = jnp.bfloat16
STATE_PARTS = 4


def silu(v):
    return v / (1.0 + jnp.exp(-v))


def sigmoid(v):
    return 1.0 / (1.0 + jnp.exp(-v))


def rms_scale(values, gain):
    values = values.astype(F32)
    return (
        values
        * lax.rsqrt(jnp.mean(values * values, axis=-1, keepdims=True) + EPS)
        * gain.astype(F32).reshape(1, -1)
    )


def unit_rows(values):
    return values * lax.rsqrt(jnp.sum(values * values, axis=-1, keepdims=True) + EPS)


def dot(a, b):
    return jnp.dot(a, b, preferred_element_type=F32)


def dot_nt(a, b):
    return lax.dot_general(a, b, (((1,), (1,)), ((), ())), preferred_element_type=F32)


def remote(src, dst, send_sem, recv_sem, e, t):
    return pltpu.make_async_remote_copy(
        src_ref=src,
        dst_ref=dst,
        send_sem=send_sem,
        recv_sem=recv_sem,
        device_id=(e, t),
        device_id_type=MESH,
    )


def loop(lo, hi, body):
    def step(i, c):
        body(i)
        return c

    lax.fori_loop(lo, hi, step, 0)


def layer_kernel(n, m, names, *refs):
    r = types.SimpleNamespace(**dict(zip(names, refs)))
    me, tp = lax.axis_index("ep"), lax.axis_index("tp")
    half = m // 2
    group = n // m
    core = lax.rem(tp, 2)
    pair = tp + 1 - 2 * core
    xi = tp // 2
    home = lax.rem(me, m)
    turn = me // m
    rows, width = r.tokens.shape
    depth, qc = r.qw_hbm.shape
    vc = r.vw_hbm.shape[1]
    key_dim, value_dim = r.new.shape[2], r.new.shape[3]
    heads = r.new.shape[1]
    keys = qc // key_dim
    share = heads // keys
    near = 2 * qc + vc
    cols = r.wide_ow.shape[1]
    hidden = r.eg_hbm.shape[2]
    quarter = width // m
    units = r.ssend2.shape[1]
    tall = group * rows

    barrier = pltpu.get_barrier_semaphore()

    steps = [
        (1 - 2 * lax.rem(me // 2**i, 2)) * 2**i for i in range(n.bit_length() - 1)
    ]

    def peer(k):
        p = me
        for i, step in enumerate(steps):
            if k >> i & 1:
                p = p + step
        return p

    cuts = (n // 2, 3 * n // 4, n), (n // 4, n // 2), (0, n // 4)
    spans = [cuts[0][:2], cuts[0][1:], cuts[1], cuts[2]]
    order = [k for lo, hi in spans for k in range(lo, hi) if k]

    for k in order:
        pl.semaphore_signal(barrier, inc=1, device_id=(peer(k), tp), device_id_type=MESH)
    for i in range(1, m):
        pl.semaphore_signal(
            barrier, inc=1, device_id=(me, lax.rem(tp + i, m)), device_id_type=MESH
        )

    fetches, alone = {}, []

    def fetch(name, src, dst, sem=None):
        if sem is None:
            sem = r.wsem.at[len(alone)]
            alone.append(name)
        c = pltpu.make_async_copy(src, dst, sem)
        c.start()
        fetches[name] = c

    for name in ("tokens", "gain"):
        fetch(name, getattr(r, name + "_hbm"), getattr(r, name))
    at = 0
    for name in ("qw", "kw", "vw", "gw"):
        src = getattr(r, name + "_hbm")
        fetch(name, src, r.weights.at[:, pl.ds(at, src.shape[1])], r.psem.at[0])
        at += src.shape[1]
    for name in ("routes", "rw", "sd", "beta", "decay", "rate", "bias", "sg", "su"):
        fetch(name, getattr(r, name + "_hbm"), getattr(r, name))
    part = rows // STATE_PARTS
    for i in range(STATE_PARTS):
        these = pl.ds(i * part, part)
        fetch(("state", i), r.state_hbm.at[these], r.new.at[these], r.psem.at[1])
    for name in ("head_gain", "ffn_gain", "bg"):
        fetch(name, getattr(r, name + "_hbm"), getattr(r, name))
    own_ow = pl.ds(pl.multiple_of(tp * vc, vc), vc)
    mine = pl.ds(pl.multiple_of(core * hidden, hidden), hidden)
    other = pl.ds(pl.multiple_of((1 - core) * hidden, hidden), hidden)
    fetch("ow", r.ow_hbm, r.wide_ow.at[own_ow])
    mine_up = pl.ds(pl.multiple_of((2 + core) * hidden, hidden), hidden)
    other_up = pl.ds(pl.multiple_of((3 - core) * hidden, hidden), hidden)
    fetch("eg", r.eg_hbm.at[0], r.egu.at[:, mine])
    fetch("eu", r.eu_hbm.at[0], r.egu.at[:, mine_up])
    fetch("ed", r.ed_hbm.at[0], r.ed.at[mine])

    def arrived(ref, sem):
        remote(ref, ref, sem, sem, me, pair).wait_recv()

    def left(ref, sem):
        remote(ref, ref, sem, sem, me, pair).wait_send()

    fetches["tokens"].wait()
    fetches["gain"].wait()
    tokens = r.tokens[...]
    normed = rms_scale(tokens, r.gain[...]).astype(BF16)
    for e in range(n):
        r.xsend[e] = normed[:, e * depth : (e + 1) * depth]
        r.tsend[e] = tokens[:, e * depth : (e + 1) * depth]

    fetches["routes"].wait()
    fetches["rw"].wait()
    rw = r.rw[...]
    scaled = rw / jnp.sum(rw, axis=0, keepdims=True) * ROUTED_SCALE
    routes = r.routes[...]
    expert = lax.broadcasted_iota(jnp.int32, (128, rows), 0)
    by_expert = jnp.zeros((128, rows), F32)
    for k in range(routes.shape[0]):
        by_expert = by_expert + jnp.where(
            expert == routes[k : k + 1, :], scaled[k : k + 1, :], 0.0
        )
    by_expert = by_expert.T
    lane = lax.broadcasted_iota(jnp.int32, (rows, 128), 1)
    for e in range(n):
        w = by_expert[:, e : e + 1]
        high = w.astype(BF16).astype(F32)
        r.csend[e] = jnp.where(lane < 64, high, w - high).astype(BF16)
    fetches["sd"].wait()
    for e in range(n):
        r.ssend2[e] = r.sd[e * units : (e + 1) * units]
    pl.semaphore_wait(barrier, n + m - 2)

    for g, (lo, hi) in enumerate(spans):
        for k in range(max(lo, 1), hi):
            p = peer(k)
            remote(r.xsend.at[p], r.xbuf.at[k], r.xs.at[0], r.xr.at[g], p, tp).start()
    r.xbuf[0] = r.xsend[me]
    def send_shared(src, dst, s, d):
        for k in order:
            p = peer(k)
            remote(src.at[p], dst.at[core, me], s.at[0], d.at[0], p, tp).start()
        dst[core, me] = src[me]

    send_shared(r.ssend2, r.sbuf2, r.s2s, r.s2r)

    for i in range(1, m):
        t = lax.rem(tp + i, m)
        remote(r.ow_hbm, r.wide_ow.at[own_ow], r.ows.at[0], r.owr.at[0], me, t).start()
    e_copies = [
        remote(r.eg_hbm.at[0], r.egu.at[:, mine], r.es.at[0], r.er.at[0], me, pair),
        remote(r.eu_hbm.at[0], r.egu.at[:, mine_up], r.es.at[1], r.er.at[1], me, pair),
        remote(r.ed_hbm.at[0], r.ed.at[mine], r.es.at[2], r.er.at[2], me, pair),
    ]
    for c in e_copies:
        c.start()

    for name in ("beta", "decay", "rate", "bias", "sg", "su"):
        fetches[name].wait()
    column = lax.broadcasted_iota(jnp.int32, (rows, r.beta.shape[0]), 1)

    def own_heads(w):
        logits = dot_nt(normed, w)
        return [
            jnp.sum(jnp.where(column == tp * heads + h, logits, 0.0), axis=1, keepdims=True)
            for h in range(heads)
        ]

    def wide(v):
        return jnp.broadcast_to(v, (rows, value_dim))

    beta = own_heads(r.beta[...])
    decay = own_heads(r.decay[...])
    for h in range(heads):
        at = slice(h * value_dim, (h + 1) * value_dim)
        strength = sigmoid(wide(beta[h]))
        shifted = wide(decay[h]) + r.bias[:, h : h + 1]
        softplus = jnp.maximum(shifted, 0.0) + jnp.log1p(jnp.exp(-jnp.abs(shifted)))
        retain = jnp.exp(-r.rate[:, h : h + 1] * softplus)
        r.retain[:, at] = retain
        r.pull[:, at] = strength * retain
        r.push[:, at] = strength
    for at, name in enumerate(("sg", "su")):
        by_unit = getattr(r, name)[...].astype(F32).T.astype(BF16)
        for e in range(n):
            r.ssend1[e, at * units : (at + 1) * units] = by_unit[e * units : (e + 1) * units]

    pltpu.make_async_copy(r.weights, r.weights, r.psem.at[0]).wait()
    for g, (lo, hi) in enumerate(spans):
        if hi > max(lo, 1):
            arrived(r.xbuf.at[pl.ds(max(lo, 1), hi - max(lo, 1))], r.xr.at[g])
        x = r.xbuf[lo:hi].reshape((hi - lo) * rows, depth)
        for c in range(0, near, 512):
            size = min(512, near - c)
            out = dot(x, r.weights[:, c : c + size])
            r.asend[lo:hi, :, c : c + size] = out.astype(BF16).reshape(hi - lo, rows, size)
        for k in range(lo + 1, hi, 2):
            remote(
                r.asend.at[k, :, pl.ds(2 * qc, vc)],
                r.vpart.at[k // 2],
                r.us.at[0],
                r.ur.at[g],
                peer(1),
                tp,
            ).start()
        for k in range(max(lo, 1), hi):
            remote(
                r.asend.at[k, :, pl.ds(0, 2 * qc)],
                r.abuf.at[k],
                r.as_.at[0],
                r.ar.at[0],
                peer(k),
                tp,
            ).start()
    r.abuf[0] = r.asend[0, :, : 2 * qc]
    x = r.xbuf[...].reshape(n * rows, depth)
    out = dot(x, r.weights[:, near:])
    r.bsend[...] = out.astype(BF16).reshape(n, rows, vc)
    for k in order:
        if k % 2:
            remote(
                r.bsend.at[k], r.gpart.at[k // 2], r.ws.at[0], r.wr.at[0], peer(1), tp
            ).start()

    at_home = tp == home

    @pl.when(at_home)
    def _():
        for k in order:
            p = peer(k)
            remote(
                r.tsend.at[p], r.tbuf.at[turn], r.ts.at[0], r.tr.at[0], p, tp
            ).start()
        r.tbuf[turn] = r.tsend[me]

    def send_on(k, own, part, src, dst, sent, got):
        both = (own.astype(F32) + part[k].astype(F32)).astype(BF16)
        if k == 0:
            dst[0] = both
        else:
            src[k] = both
            remote(src.at[k], dst.at[k], sent.at[0], got.at[0], peer(2 * k), tp).start()

    for g, (lo, hi) in enumerate(spans):
        arrived(r.vpart.at[pl.ds(lo // 2, (hi - lo) // 2)], r.ur.at[g])
        for k in range(lo // 2, hi // 2):
            own = r.asend[2 * k, :, 2 * qc :]
            send_on(k, own, r.vpart, r.vsend, r.vbuf, r.vs, r.vr)
    arrived(r.gpart, r.wr.at[0])
    for lo, hi in spans:
        for k in range(lo // 2, hi // 2):
            send_on(k, r.bsend[2 * k], r.gpart, r.gsend, r.gbuf, r.bs, r.br)

    for name in ("head_gain", "ffn_gain", "bg"):
        fetches[name].wait()
    gain = r.ffn_gain[...].astype(F32).reshape(1, -1)
    bg = r.bg[...].astype(F32).reshape(1, -1)
    for e in range(n):
        r.gains[e] = gain[:, e * cols : (e + 1) * cols]
        r.bgs[e] = bg[:, e * cols : (e + 1) * cols]
    pltpu.make_async_copy(r.new, r.new, r.psem.at[1]).wait()

    arrived(r.abuf.at[pl.ds(1, n - 1)], r.ar.at[0])
    arrived(r.vbuf.at[pl.ds(1, n // 2 - 1)], r.vr.at[0])

    def gathered(ref, c, size):
        acc = ref[0, :, c : c + size].astype(F32)
        for e in range(1, ref.shape[0]):
            acc = acc + ref[e, :, c : c + size].astype(F32)
        return acc.astype(BF16).astype(F32)

    q_rows = [
        unit_rows(silu(gathered(r.abuf, j * key_dim, key_dim))) * key_dim ** (-0.5)
        for j in range(keys)
    ]
    k_rows = [
        unit_rows(silu(gathered(r.abuf, qc + j * key_dim, key_dim))) for j in range(keys)
    ]
    for h in range(heads):
        at = slice(h * value_dim, (h + 1) * value_dim)
        r.push[:, at] = r.push[:, at] * silu(
            gathered(r.vbuf, h * value_dim, value_dim)
        )
    for j in range(keys):
        r.qk[:, j * value_dim : (j + 1) * value_dim] = wide(
            jnp.sum(q_rows[j] * k_rows[j], axis=1, keepdims=True)
        )
    stacked = q_rows + k_rows
    stacked.append(jnp.zeros((128 - 2 * keys * rows, key_dim), F32))
    r.kq[...] = jnp.concatenate(stacked, axis=0).T

    for j in range(keys):
        for s in range(rows):
            q = jnp.broadcast_to(r.kq[:, j * rows + s : j * rows + s + 1], (key_dim, value_dim))
            at = (keys + j) * rows + s
            k = jnp.broadcast_to(r.kq[:, at : at + 1], (key_dim, value_dim))
            one = slice(s, s + 1)
            qk = r.qk[one, j * value_dim : (j + 1) * value_dim]
            for h in range(j * share, (j + 1) * share):
                c = slice(h * value_dim, (h + 1) * value_dim)
                state = r.new[s, h]
                retain = r.retain[one, c]
                predicted = jnp.sum(state * k, axis=0, keepdims=True)
                before = jnp.sum(state * q, axis=0, keepdims=True)
                correction = r.push[one, c] - r.pull[one, c] * predicted
                r.new[s, h] = state * retain + k * correction
                r.held[one, c] = before * retain + qk * correction

    arrived(r.gbuf.at[pl.ds(1, n // 2 - 1)], r.br.at[0])
    for h in range(heads):
        c = slice(h * value_dim, (h + 1) * value_dim)
        gate = silu(gathered(r.gbuf, h * value_dim, value_dim))
        r.hsend[:, c] = (rms_scale(r.held[:, c], r.head_gain[...]) * gate).astype(BF16)

    def send_h(p):
        remote(
            r.hsend, r.hbuf.at[turn * m + tp], r.hs.at[0], r.hr.at[0], p, home
        ).start()

    for k in order:
        send_h(peer(k))

    @pl.when(jnp.logical_not(at_home))
    def _():
        send_h(me)

    @pl.when(at_home)
    def _():
        r.hbuf[turn * m + tp] = r.hsend[...]

    send_shared(r.ssend1, r.sbuf1, r.s1s, r.s1r)
    for k in order:
        p = peer(k)
        remote(r.csend.at[p], r.cbuf.at[me], r.cs.at[0], r.cr.at[0], p, tp).start()
    r.cbuf[me] = r.csend[me]

    fetches["ow"].wait()
    arrived(r.wide_ow.at[pl.ds(0, (m - 1) * vc)], r.owr.at[0])

    @pl.when(at_home)
    def _():
        arrived(r.tbuf.at[pl.ds(0, group - 1)], r.tr.at[0])
        arrived(r.hbuf.at[pl.ds(0, n - 1)], r.hr.at[0])

    @pl.when(jnp.logical_not(at_home))
    def _():
        arrived(r.tbuf, r.tr.at[0])
        arrived(r.hbuf, r.hr.at[0])

    residual = r.tbuf[...].reshape(tall, cols).astype(F32)
    mix = None
    for t in range(m):
        h = jnp.concatenate([r.hbuf[b * m + t] for b in range(group)], axis=0)
        term = dot(h, r.wide_ow[t * vc : (t + 1) * vc])
        mix = term if mix is None else mix + term
    r.resid[xi, me] = (residual + mix).astype(BF16).reshape(group, rows, cols)

    mine_resid = r.resid.at[xi, me]
    for k in order:
        remote(mine_resid, mine_resid, r.fs.at[0], r.fr.at[k], peer(k), tp).start()

    def f_pass(k):
        ref = r.resid.at[xi, peer(k)]
        sem = r.gr.at[xi, 2 * k // n]
        for i in range(1, half):
            t = 2 * lax.rem(xi + i, half) + core
            remote(ref, ref, r.gs.at[0], sem, me, t).start()

    f_pass(0)

    for name in ("eg", "eu", "ed"):
        fetches[name].wait()
    for i, ref in enumerate((r.egu.at[:, other], r.egu.at[:, other_up], r.ed.at[other])):
        arrived(ref, r.er.at[i])

    class Sums:
        up = square = branch = 0.0
        dense = [0.0, 0.0]

    def scaled_block(a, p):
        v = r.resid[a, p].reshape(tall, cols).astype(F32)
        return v, (v * r.gains[p]).astype(BF16)

    def absorb(sums, a, p):
        v, u = scaled_block(a, p)
        at = pl.ds(pl.multiple_of(p * cols, cols), cols)
        sums.square = sums.square + v * v
        sums.branch = sums.branch + u.astype(F32) * r.bgs[p]
        sums.up = sums.up + dot(u, r.egu[at])

    def absorb_dense(sums, a, p):
        u = scaled_block(a, p)[1]
        sums.dense = [d + dot_nt(u, r.sbuf1[c, p]) for c, d in enumerate(sums.dense)]

    first = Sums()
    absorb(first, xi, me)
    arrived(r.sbuf1.at[0, pl.ds(0, n - 1)], r.s1r.at[0])
    s_copies = [remote(r.sbuf1.at[core], r.sbuf1.at[core], r.ps.at[0], r.pr.at[0], me, pair)]
    s_copies[0].start()
    arrived(r.sbuf2.at[0, pl.ds(0, n - 1)], r.s2r.at[0])
    s_copies.append(
        remote(r.sbuf2.at[core], r.sbuf2.at[core], r.ps.at[1], r.pr.at[1], me, pair)
    )
    s_copies[1].start()
    for k in range(1, n // 2):
        arrived(r.resid.at[xi, peer(k)], r.fr.at[k])
        f_pass(k)
        absorb(first, xi, peer(k))
    arrived(r.sbuf1.at[0], r.pr.at[0])
    arrived(r.sbuf2.at[0], r.pr.at[1])
    for c in range(2):
        r.shared[c] = jnp.concatenate([r.sbuf2[c, e] for e in range(n)], axis=1)
    for k in range(n // 2):
        absorb_dense(first, xi, peer(k))
    for k in range(n // 2, n):
        arrived(r.resid.at[xi, peer(k)], r.fr.at[k])
        f_pass(k)
        absorb(first, xi, peer(k))
        absorb_dense(first, xi, peer(k))
    arrived(r.cbuf.at[pl.ds(0, n - 1)], r.cr.at[0])
    for a in range(half):
        for b in range(group):
            w = r.cbuf[b * m + 2 * a + core].astype(F32)
            r.routed[a, b * rows : (b + 1) * rows] = jnp.broadcast_to(
                w[:, 0:1] + w[:, 64:65], (rows, 128)
            )
    upper = me // (n // 2)

    def target(a, b):
        return b * m + 2 * a + core

    def away(a, b, q):
        return jnp.logical_or(target(a, b) != me, q != tp)

    def finish(sums, a):
        square = jnp.sum(sums.square, axis=1, keepdims=True)
        scale = lax.rsqrt(square / width + EPS)
        up = sums.up * scale
        act = (silu(up[:, : 2 * hidden]) * up[:, 2 * hidden :]).astype(BF16)
        dense = []
        for d in sums.dense:
            both = d * scale
            dense.append((silu(both[:, :units]) * both[:, units:]).astype(BF16))
        branch = sigmoid(jnp.sum(sums.branch, axis=1, keepdims=True) * scale)
        weight = r.routed[a, :, 0:1]
        for k in range(m):
            q = 2 * lax.rem(xi + k // 2, half) + lax.rem(core + k, 2)
            at = pl.ds(pl.multiple_of(q * quarter, quarter), quarter)
            out = weight * dot(act, r.ed[:, at])
            side = dot(dense[0], r.shared[0, :, at])
            side = side + dot(dense[1], r.shared[1, :, at])
            r.rsend[a, :, q] = (out + branch * side).astype(BF16).reshape(group, rows, quarter)
            for i in range(group):
                b = lax.rem(i + (group // 2) * (1 - upper), group)

                @pl.when(away(a, b, q))
                def _():
                    remote(
                        r.rsend.at[a, b, q],
                        r.rbuf.at[me * half + xi],
                        r.rs.at[0],
                        r.rr.at[0],
                        target(a, b),
                        q,
                    ).start()

    finish(first, xi)
    for i in range(1, half):
        a = lax.rem(xi + i, half)
        second = Sums()
        for g in range(2):
            arrived(r.resid.at[a, pl.ds(0, n // 2)], r.gr.at[a, g])
            for k in range(g * n // 2, (g + 1) * n // 2):
                absorb(second, a, peer(k))
                absorb_dense(second, a, peer(k))
        finish(second, a)

    held_here = core == lax.rem(home, 2)
    place = home // 2
    d_copy = remote(
        r.resid.at[place, pl.ds(pair * group, group), turn],
        r.rown,
        r.ds.at[0],
        r.dr.at[0],
        me,
        pair,
    )

    @pl.when(held_here)
    def _():
        d_copy.start()
        r.rown[...] = r.resid[place, pl.ds(tp * group, group), turn]
        r.rbuf[me * half + xi] = r.rsend[place, turn, tp]

    left(r.xbuf.at[pl.ds(0, n - 1)], r.xs.at[0])
    left(r.cbuf.at[pl.ds(0, n - 1)], r.cs.at[0])
    left(r.abuf.at[pl.ds(0, n - 1)], r.as_.at[0])
    left(r.vpart, r.us.at[0])
    left(r.gpart, r.ws.at[0])
    left(r.vbuf.at[pl.ds(0, n // 2 - 1)], r.vs.at[0])
    left(r.gbuf.at[pl.ds(0, n // 2 - 1)], r.bs.at[0])
    left(r.sbuf1.at[0, pl.ds(0, n - 1)], r.s1s.at[0])
    left(r.sbuf2.at[0, pl.ds(0, n - 1)], r.s2s.at[0])
    left(r.resid.at[0, pl.ds(0, n - 1)], r.fs.at[0])
    if half > 1:
        left(r.resid.at[pl.ds(0, half - 1)], r.gs.at[0])
    left(r.wide_ow.at[pl.ds(0, (m - 1) * vc)], r.ows.at[0])
    for c in e_copies + s_copies:
        c.wait_send()

    @pl.when(at_home)
    def _():
        left(r.tsend.at[pl.ds(0, n - 1)], r.ts.at[0])
        left(r.hbuf.at[pl.ds(0, n - 1)], r.hs.at[0])

    @pl.when(jnp.logical_not(at_home))
    def _():
        left(r.hbuf, r.hs.at[0])

    @pl.when(held_here)
    def _():
        arrived(r.rbuf.at[pl.ds(0, n * half - 1)], r.rr.at[0])

    @pl.when(jnp.logical_not(held_here))
    def _():
        arrived(r.rbuf, r.rr.at[0])
        arrived(r.rown, r.dr.at[0])

    acc = jnp.concatenate([r.rown[b].astype(F32) for b in range(group)], axis=1)
    for p in range(n * half):
        acc = acc + r.rbuf[p].astype(F32)
    r.obuf[tp] = acc.astype(BF16)
    for i in range(1, m):
        t = lax.rem(tp + i, m)
        remote(r.obuf.at[tp], r.obuf.at[tp], r.os_.at[0], r.or_.at[0], me, t).start()

    @pl.when(held_here)
    def _():
        d_copy.wait_send()
        left(r.rbuf.at[pl.ds(0, n * half - 1)], r.rs.at[0])

    @pl.when(jnp.logical_not(held_here))
    def _():
        left(r.rbuf, r.rs.at[0])

    arrived(r.obuf.at[pl.ds(0, m - 1)], r.or_.at[0])
    for t in range(m):
        r.out[:, t * quarter : (t + 1) * quarter] = r.obuf[t]
    left(r.obuf.at[pl.ds(0, m - 1)], r.os_.at[0])


def flush_kernel(layer_ref, state_ref, layer_out, state_out, sem):
    rows = state_ref.shape[0]
    part = rows // STATE_PARTS
    copies = [pltpu.make_async_copy(layer_ref, layer_out, sem.at[STATE_PARTS])]
    for i in range(STATE_PARTS):
        these = pl.ds(i * part, part)
        copies.append(
            pltpu.make_async_copy(state_ref.at[these], state_out.at[these], sem.at[i])
        )
    for c in copies:
        c.start()
    for c in copies:
        c.wait()


VMEM = pl.BlockSpec(memory_space=pltpu.VMEM)
HBM = pl.BlockSpec(memory_space=pltpu.HBM)


def per_device(
    n,
    m,
    tokens,
    norm_gain,
    query_weight,
    key_weight,
    value_weight,
    outgate_weight,
    beta_weight,
    decay_weight,
    decay_rate,
    decay_bias,
    head_gain,
    recurrent,
    output_weight,
    ffn_gain,
    routes,
    route_weight,
    expert_gate,
    expert_up,
    expert_down,
    shared_gate,
    shared_up,
    shared_down,
    branch_gate,
):
    rows, width = tokens.shape
    _, heads, key_dim, value_dim = recurrent.shape
    depth, qc = query_weight.shape
    vc = value_weight.shape[1]
    keys = qc // key_dim
    near = 2 * qc + vc
    half = m // 2
    group = n // m
    units = shared_gate.shape[1] // n
    cols = shared_down.shape[1]
    hidden = expert_gate.shape[2]
    quarter = width // m
    sds = jax.ShapeDtypeStruct
    dma = pltpu.SemaphoreType.DMA

    inputs = dict(
        tokens=tokens,
        gain=norm_gain,
        qw=query_weight,
        kw=key_weight,
        vw=value_weight,
        gw=outgate_weight,
        beta=beta_weight.T,
        decay=decay_weight.T,
        rate=decay_rate[None, :],
        bias=decay_bias[None, :],
        routes=routes.T,
        rw=route_weight.T,
        head_gain=head_gain,
        state=recurrent,
        ow=output_weight,
        ffn_gain=ffn_gain,
        eg=expert_gate,
        eu=expert_up,
        ed=expert_down,
        sg=shared_gate,
        su=shared_up,
        sd=shared_down,
        bg=branch_gate,
    )
    plain = ("tokens", "gain", "beta", "decay", "rate", "bias", "routes", "rw")
    plain += ("head_gain", "ffn_gain", "sg", "su", "sd", "bg")
    scratch = {k: pltpu.VMEM(inputs[k].shape, inputs[k].dtype) for k in plain}
    scratch.update(
        weights=pltpu.VMEM((depth, near + vc), BF16),
        wide_ow=pltpu.VMEM((m * vc, cols), BF16),
        egu=pltpu.VMEM((width, 4 * hidden), BF16),
        gains=pltpu.VMEM((n, 1, cols), F32),
        bgs=pltpu.VMEM((n, 1, cols), F32),
        ed=pltpu.VMEM((2 * hidden, width), BF16),
        xsend=pltpu.VMEM((n, rows, depth), BF16),
        xbuf=pltpu.VMEM((n, rows, depth), BF16),
        csend=pltpu.VMEM((n, rows, 128), BF16),
        cbuf=pltpu.VMEM((n, rows, 128), BF16),
        tsend=pltpu.VMEM((n, rows, depth), BF16),
        tbuf=pltpu.VMEM((group, rows, depth), BF16),
        ssend1=pltpu.VMEM((n, 2 * units, cols), BF16),
        sbuf1=pltpu.VMEM((2, n, 2 * units, cols), BF16),
        ssend2=pltpu.VMEM((n, units, cols), BF16),
        sbuf2=pltpu.VMEM((2, n, units, cols), BF16),
        shared=pltpu.VMEM((2, units, width), BF16),
        asend=pltpu.VMEM((n, rows, near), BF16),
        abuf=pltpu.VMEM((n, rows, 2 * qc), BF16),
        bsend=pltpu.VMEM((n, rows, vc), BF16),
        vpart=pltpu.VMEM((n // 2, rows, vc), BF16),
        vsend=pltpu.VMEM((n // 2, rows, vc), BF16),
        vbuf=pltpu.VMEM((n // 2, rows, vc), BF16),
        gpart=pltpu.VMEM((n // 2, rows, vc), BF16),
        gsend=pltpu.VMEM((n // 2, rows, vc), BF16),
        gbuf=pltpu.VMEM((n // 2, rows, vc), BF16),
        retain=pltpu.VMEM((rows, vc), F32),
        pull=pltpu.VMEM((rows, vc), F32),
        push=pltpu.VMEM((rows, vc), F32),
        qk=pltpu.VMEM((rows, keys * value_dim), F32),
        kq=pltpu.VMEM((key_dim, 128), F32),
        held=pltpu.VMEM((rows, vc), F32),
        routed=pltpu.VMEM((half, group * rows, 128), F32),
        hsend=pltpu.VMEM((rows, vc), BF16),
        hbuf=pltpu.VMEM((n, rows, vc), BF16),
        resid=pltpu.VMEM((half, n, group, rows, cols), BF16),
        rown=pltpu.VMEM((group, rows, cols), BF16),
        rsend=pltpu.VMEM((half, group, m, rows, quarter), BF16),
        rbuf=pltpu.VMEM((n * half, rows, quarter), BF16),
        obuf=pltpu.VMEM((m, rows, quarter), BF16),
        wsem=dma((len(inputs) - 5,)),
        psem=dma((2,)),
    )
    counts = dict(xr=4, ur=4, fr=n, es=3, er=3, ps=2, pr=2)
    for name in ("x", "c", "ow", "a", "u", "w", "v", "b", "t", "s1", "s2", "h", "f", "g", "e", "p", "d", "r", "o"):
        for end in ("s", "r"):
            key = {"as": "as_", "os": "os_", "or": "or_"}.get(name + end, name + end)
            scratch[key] = dma((counts.get(key, 1),))
    scratch["gr"] = dma((half, 2))
    names = [k + "_hbm" for k in inputs] + ["out", "new"] + list(scratch)
    layer, state = pl.pallas_call(
        functools.partial(layer_kernel, n, m, names),
        out_shape=(pltpu.VMEM((rows, width), BF16), pltpu.VMEM(recurrent.shape, F32)),
        in_specs=[HBM] * len(inputs),
        out_specs=(VMEM, VMEM),
        scratch_shapes=list(scratch.values()),
        compiler_params=pltpu.CompilerParams(
            collective_id=0, has_side_effects=True, vmem_limit_bytes=48 * 2**20
        ),
    )(*(pltpu.with_memory_space_constraint(v, pltpu.HBM) for v in inputs.values()))

    return pl.pallas_call(
        flush_kernel,
        out_shape=(sds((rows, width), BF16), sds(recurrent.shape, F32)),
        in_specs=[VMEM, VMEM],
        out_specs=(HBM, HBM),
        scratch_shapes=[dma((STATE_PARTS + 1,))],
        compiler_params=pltpu.CompilerParams(vmem_limit_bytes=4 * 2**20),
    )(layer, state)


def solution(mesh):
    return jax.shard_map(
        functools.partial(per_device, mesh.shape["ep"], mesh.shape["tp"]),
        mesh=mesh,
        in_specs=(
            P("ep", None),
            P(),
            P("ep", "tp"),
            P("ep", "tp"),
            P("ep", "tp"),
            P("ep", "tp"),
            P(),
            P(),
            P("tp"),
            P("tp"),
            P(),
            P("ep", "tp", None, None),
            P("tp", "ep"),
            P(),
            P("ep", None),
            P("ep", None),
            P("ep", None, "tp"),
            P("ep", None, "tp"),
            P("ep", "tp", None),
            P("ep", "tp"),
            P("ep", "tp"),
            P("tp", "ep"),
            P(),
        ),
        out_specs=(P("ep", None), P("ep", "tp", None, None)),
        check_vma=False,
    )
```

```python
import functools
import types

import jax
import jax.numpy as jnp
from jax import lax
from jax.experimental import pallas as pl
from jax.experimental.pallas import tpu as pltpu
from jax.sharding import PartitionSpec as P

EPS = 1e-06
ROUTED_SCALE = 2.5
MESH = pl.DeviceIdType.MESH
F32 = jnp.float32
BF16 = jnp.bfloat16
STATE_PARTS = 4


def silu(v):
    return v / (1.0 + jnp.exp(-v))


def sigmoid(v):
    return 1.0 / (1.0 + jnp.exp(-v))


def rms_scale(values, gain):
    values = values.astype(F32)
    return (
        values
        * lax.rsqrt(jnp.mean(values * values, axis=-1, keepdims=True) + EPS)
        * gain.astype(F32).reshape(1, -1)
    )


def unit_rows(values):
    return values * lax.rsqrt(jnp.sum(values * values, axis=-1, keepdims=True) + EPS)


def dot(a, b):
    return jnp.dot(a, b, preferred_element_type=F32)


def dot_nt(a, b):
    return lax.dot_general(a, b, (((1,), (1,)), ((), ())), preferred_element_type=F32)


def remote(src, dst, send_sem, recv_sem, e, t):
    return pltpu.make_async_remote_copy(
        src_ref=src,
        dst_ref=dst,
        send_sem=send_sem,
        recv_sem=recv_sem,
        device_id=(e, t),
        device_id_type=MESH,
    )


def loop(lo, hi, body):
    def step(i, c):
        body(i)
        return c

    lax.fori_loop(lo, hi, step, 0)


def layer_kernel(n, m, names, *refs):
    r = types.SimpleNamespace(**dict(zip(names, refs)))
    me, tp = lax.axis_index("ep"), lax.axis_index("tp")
    half = m // 2
    group = n // m
    core = lax.rem(tp, 2)
    pair = tp + 1 - 2 * core
    xi = tp // 2
    home = lax.rem(me, m)
    turn = me // m
    rows, width = r.tokens.shape
    depth, qc = r.qw_hbm.shape
    vc = r.vw_hbm.shape[1]
    key_dim, value_dim = r.new.shape[2], r.new.shape[3]
    heads = r.new.shape[1]
    keys = qc // key_dim
    share = heads // keys
    total = 2 * qc + 2 * vc
    cols = r.wide_ow.shape[1]
    hidden = r.eg_hbm.shape[2]
    quarter = width // m
    units = r.ssend2.shape[1]
    tall = group * rows

    barrier = pltpu.get_barrier_semaphore()

    steps = [
        (1 - 2 * lax.rem(me // 2**i, 2)) * 2**i for i in range(n.bit_length() - 1)
    ]

    def peer(k):
        p = me
        for i, step in enumerate(steps):
            if k >> i & 1:
                p = p + step
        return p

    cuts = (n // 2, 3 * n // 4, n), (n // 4, n // 2), (0, n // 4)
    spans = [cuts[0][:2], cuts[0][1:], cuts[1], cuts[2]]
    order = [k for lo, hi in spans for k in range(lo, hi) if k]

    for k in order:
        pl.semaphore_signal(barrier, inc=1, device_id=(peer(k), tp), device_id_type=MESH)
    for i in range(1, m):
        pl.semaphore_signal(
            barrier, inc=1, device_id=(me, lax.rem(tp + i, m)), device_id_type=MESH
        )

    fetches, alone = {}, []

    def fetch(name, src, dst, sem=None):
        if sem is None:
            sem = r.wsem.at[len(alone)]
            alone.append(name)
        c = pltpu.make_async_copy(src, dst, sem)
        c.start()
        fetches[name] = c

    for name in ("tokens", "gain"):
        fetch(name, getattr(r, name + "_hbm"), getattr(r, name))
    at = 0
    for name in ("qw", "kw", "vw", "gw"):
        src = getattr(r, name + "_hbm")
        fetch(name, src, r.weights.at[:, pl.ds(at, src.shape[1])], r.psem.at[0])
        at += src.shape[1]
    for name in ("routes", "rw", "sd", "beta", "decay", "rate", "bias", "sg", "su"):
        fetch(name, getattr(r, name + "_hbm"), getattr(r, name))
    part = rows // STATE_PARTS
    for i in range(STATE_PARTS):
        these = pl.ds(i * part, part)
        fetch(("state", i), r.state_hbm.at[these], r.new.at[these], r.psem.at[1])
    for name in ("head_gain", "ffn_gain", "bg"):
        fetch(name, getattr(r, name + "_hbm"), getattr(r, name))
    own_ow = pl.ds(pl.multiple_of(tp * vc, vc), vc)
    mine = pl.ds(pl.multiple_of(core * hidden, hidden), hidden)
    other = pl.ds(pl.multiple_of((1 - core) * hidden, hidden), hidden)
    fetch("ow", r.ow_hbm, r.wide_ow.at[own_ow])
    mine_up = pl.ds(pl.multiple_of((2 + core) * hidden, hidden), hidden)
    other_up = pl.ds(pl.multiple_of((3 - core) * hidden, hidden), hidden)
    fetch("eg", r.eg_hbm.at[0], r.egu.at[:, mine])
    fetch("eu", r.eu_hbm.at[0], r.egu.at[:, mine_up])
    fetch("ed", r.ed_hbm.at[0], r.ed.at[mine])

    def arrived(ref, sem):
        remote(ref, ref, sem, sem, me, pair).wait_recv()

    def left(ref, sem):
        remote(ref, ref, sem, sem, me, pair).wait_send()

    fetches["tokens"].wait()
    fetches["gain"].wait()
    tokens = r.tokens[...]
    normed = rms_scale(tokens, r.gain[...]).astype(BF16)
    for e in range(n):
        r.xsend[e] = normed[:, e * depth : (e + 1) * depth]
        r.tsend[e] = tokens[:, e * depth : (e + 1) * depth]

    fetches["routes"].wait()
    fetches["rw"].wait()
    rw = r.rw[...]
    scaled = rw / jnp.sum(rw, axis=0, keepdims=True) * ROUTED_SCALE
    routes = r.routes[...]
    expert = lax.broadcasted_iota(jnp.int32, (128, rows), 0)
    by_expert = jnp.zeros((128, rows), F32)
    for k in range(routes.shape[0]):
        by_expert = by_expert + jnp.where(
            expert == routes[k : k + 1, :], scaled[k : k + 1, :], 0.0
        )
    by_expert = by_expert.T
    lane = lax.broadcasted_iota(jnp.int32, (rows, 128), 1)
    for e in range(n):
        w = by_expert[:, e : e + 1]
        high = w.astype(BF16).astype(F32)
        r.csend[e] = jnp.where(lane < 64, high, w - high).astype(BF16)
    fetches["sd"].wait()
    for e in range(n):
        r.ssend2[e] = r.sd[e * units : (e + 1) * units]
    pl.semaphore_wait(barrier, n + m - 2)

    for g, (lo, hi) in enumerate(spans):
        for k in range(max(lo, 1), hi):
            p = peer(k)
            remote(r.xsend.at[p], r.xbuf.at[k], r.xs.at[0], r.xr.at[g], p, tp).start()
    r.xbuf[0] = r.xsend[me]
    def send_shared(src, dst, s, d):
        for k in order:
            p = peer(k)
            remote(src.at[p], dst.at[core, me], s.at[0], d.at[0], p, tp).start()
        dst[core, me] = src[me]

    send_shared(r.ssend2, r.sbuf2, r.s2s, r.s2r)

    for i in range(1, m):
        t = lax.rem(tp + i, m)
        remote(r.ow_hbm, r.wide_ow.at[own_ow], r.ows.at[0], r.owr.at[0], me, t).start()
    e_copies = [
        remote(r.eg_hbm.at[0], r.egu.at[:, mine], r.es.at[0], r.er.at[0], me, pair),
        remote(r.eu_hbm.at[0], r.egu.at[:, mine_up], r.es.at[1], r.er.at[1], me, pair),
        remote(r.ed_hbm.at[0], r.ed.at[mine], r.es.at[2], r.er.at[2], me, pair),
    ]
    for c in e_copies:
        c.start()

    for name in ("beta", "decay", "rate", "bias", "sg", "su"):
        fetches[name].wait()
    place_of = lax.broadcasted_iota(jnp.int32, (rows, r.beta.shape[0]), 1)

    def own_heads(w):
        logits = dot_nt(normed, w)
        return [
            jnp.sum(jnp.where(place_of == tp * heads + h, logits, 0.0), axis=1, keepdims=True)
            for h in range(heads)
        ]

    def wide(v):
        return jnp.broadcast_to(v, (rows, value_dim))

    beta = own_heads(r.beta[...])
    decay = own_heads(r.decay[...])
    for h in range(heads):
        at = slice(h * value_dim, (h + 1) * value_dim)
        strength = sigmoid(wide(beta[h]))
        shifted = wide(decay[h]) + r.bias[:, h : h + 1]
        softplus = jnp.maximum(shifted, 0.0) + jnp.log1p(jnp.exp(-jnp.abs(shifted)))
        retain = jnp.exp(-r.rate[:, h : h + 1] * softplus)
        r.retain[:, at] = retain
        r.pull[:, at] = strength * retain
        r.push[:, at] = strength
    for at, name in enumerate(("sg", "su")):
        by_unit = getattr(r, name)[...].astype(F32).T.astype(BF16)
        for e in range(n):
            r.ssend1[e, at * units : (at + 1) * units] = by_unit[e * units : (e + 1) * units]

    pltpu.make_async_copy(r.weights, r.weights, r.psem.at[0]).wait()
    for g, (lo, hi) in enumerate(spans):
        if hi > max(lo, 1):
            arrived(r.xbuf.at[pl.ds(max(lo, 1), hi - max(lo, 1))], r.xr.at[g])
        x = r.xbuf[lo:hi].reshape((hi - lo) * rows, depth)
        for c in range(0, total, 512):
            size = min(512, total - c)
            out = dot(x, r.weights[:, c : c + size])
            r.asend[lo:hi, :, c : c + size] = out.astype(BF16).reshape(hi - lo, rows, size)
        for k in range(lo + 1, hi, 2):
            remote(
                r.asend.at[k, :, pl.ds(2 * qc, 2 * vc)],
                r.part.at[k // 2],
                r.us.at[0],
                r.ur.at[g],
                peer(1),
                tp,
            ).start()
        for k in range(max(lo, 1), hi):
            remote(
                r.asend.at[k, :, pl.ds(0, 2 * qc)],
                r.abuf.at[k],
                r.as_.at[0],
                r.ar.at[0],
                peer(k),
                tp,
            ).start()
    r.abuf[0] = r.asend[0, :, : 2 * qc]

    at_home = tp == home

    @pl.when(at_home)
    def _():
        for k in order:
            p = peer(k)
            remote(
                r.tsend.at[p], r.tbuf.at[turn], r.ts.at[0], r.tr.at[0], p, tp
            ).start()
        r.tbuf[turn] = r.tsend[me]

    for g, (lo, hi) in enumerate(spans):
        arrived(r.part.at[pl.ds(lo // 2, (hi - lo) // 2)], r.ur.at[g])
        for k in range(lo // 2, hi // 2):
            own = r.asend[2 * k, :, 2 * qc :].astype(F32)
            both = (own + r.part[k].astype(F32)).astype(BF16)
            if k == 0:
                r.vbuf[0] = both
            else:
                r.vsend[k] = both
                remote(
                    r.vsend.at[k], r.vbuf.at[k], r.vs.at[0], r.vr.at[0], peer(2 * k), tp
                ).start()

    for name in ("head_gain", "ffn_gain", "bg"):
        fetches[name].wait()
    gain = r.ffn_gain[...].astype(F32).reshape(1, -1)
    bg = r.bg[...].astype(F32).reshape(1, -1)
    for e in range(n):
        r.gains[e] = gain[:, e * cols : (e + 1) * cols]
        r.bgs[e] = bg[:, e * cols : (e + 1) * cols]
    pltpu.make_async_copy(r.new, r.new, r.psem.at[1]).wait()

    arrived(r.abuf.at[pl.ds(1, n - 1)], r.ar.at[0])

    def gathered(ref, c, size):
        acc = ref[0, :, c : c + size].astype(F32)
        for e in range(1, ref.shape[0]):
            acc = acc + ref[e, :, c : c + size].astype(F32)
        return acc.astype(BF16).astype(F32)

    q_rows = [
        unit_rows(silu(gathered(r.abuf, j * key_dim, key_dim))) * key_dim ** (-0.5)
        for j in range(keys)
    ]
    k_rows = [
        unit_rows(silu(gathered(r.abuf, qc + j * key_dim, key_dim))) for j in range(keys)
    ]
    for j in range(keys):
        r.qk[:, j * value_dim : (j + 1) * value_dim] = wide(
            jnp.sum(q_rows[j] * k_rows[j], axis=1, keepdims=True)
        )
    stacked = q_rows + k_rows
    stacked.append(jnp.zeros((128 - 2 * keys * rows, key_dim), F32))
    r.kq[...] = jnp.concatenate(stacked, axis=0).T

    def column(at):
        return jnp.broadcast_to(r.kq[:, at : at + 1], (key_dim, value_dim))

    for j in range(keys):
        for s in range(rows):
            q, k = column(j * rows + s), column((keys + j) * rows + s)
            for h in range(j * share, (j + 1) * share):
                c = slice(h * value_dim, (h + 1) * value_dim)
                state = r.new[s, h]
                r.seen[s : s + 1, c] = jnp.sum(state * k, axis=0, keepdims=True)
                r.held[s : s + 1, c] = jnp.sum(state * q, axis=0, keepdims=True)

    arrived(r.vbuf.at[pl.ds(1, n // 2 - 1)], r.vr.at[0])
    for h in range(heads):
        c = slice(h * value_dim, (h + 1) * value_dim)
        j = h // share
        values = silu(gathered(r.vbuf, h * value_dim, value_dim))
        gate = silu(gathered(r.vbuf, vc + h * value_dim, value_dim))
        correction = r.push[:, c] * values - r.pull[:, c] * r.seen[:, c]
        r.seen[:, c] = correction
        qk = r.qk[:, j * value_dim : (j + 1) * value_dim]
        readout = r.held[:, c] * r.retain[:, c] + qk * correction
        r.hsend[:, c] = (rms_scale(readout, r.head_gain[...]) * gate).astype(BF16)

    def send_h(p):
        remote(
            r.hsend, r.hbuf.at[turn * m + tp], r.hs.at[0], r.hr.at[0], p, home
        ).start()

    for k in order:
        send_h(peer(k))

    @pl.when(jnp.logical_not(at_home))
    def _():
        send_h(me)

    @pl.when(at_home)
    def _():
        r.hbuf[turn * m + tp] = r.hsend[...]

    send_shared(r.ssend1, r.sbuf1, r.s1s, r.s1r)
    for k in order:
        p = peer(k)
        remote(r.csend.at[p], r.cbuf.at[me], r.cs.at[0], r.cr.at[0], p, tp).start()
    r.cbuf[me] = r.csend[me]

    for j in range(keys):
        for s in range(rows):
            k = column((keys + j) * rows + s)
            for h in range(j * share, (j + 1) * share):
                c = slice(h * value_dim, (h + 1) * value_dim)
                r.new[s, h] = (
                    r.new[s, h] * r.retain[s : s + 1, c] + k * r.seen[s : s + 1, c]
                )

    fetches["ow"].wait()
    arrived(r.wide_ow.at[pl.ds(0, (m - 1) * vc)], r.owr.at[0])

    @pl.when(at_home)
    def _():
        arrived(r.tbuf.at[pl.ds(0, group - 1)], r.tr.at[0])
        arrived(r.hbuf.at[pl.ds(0, n - 1)], r.hr.at[0])

    @pl.when(jnp.logical_not(at_home))
    def _():
        arrived(r.tbuf, r.tr.at[0])
        arrived(r.hbuf, r.hr.at[0])

    residual = r.tbuf[...].reshape(tall, cols).astype(F32)
    mix = None
    for t in range(m):
        h = jnp.concatenate([r.hbuf[b * m + t] for b in range(group)], axis=0)
        term = dot(h, r.wide_ow[t * vc : (t + 1) * vc])
        mix = term if mix is None else mix + term
    r.resid[xi, me] = (residual + mix).astype(BF16).reshape(group, rows, cols)

    mine_resid = r.resid.at[xi, me]
    for k in order:
        remote(mine_resid, mine_resid, r.fs.at[0], r.fr.at[k], peer(k), tp).start()

    def f_pass(k):
        ref = r.resid.at[xi, peer(k)]
        sem = r.gr.at[xi, 2 * k // n]
        for i in range(1, half):
            t = 2 * lax.rem(xi + i, half) + core
            remote(ref, ref, r.gs.at[0], sem, me, t).start()

    f_pass(0)

    for name in ("eg", "eu", "ed"):
        fetches[name].wait()
    for i, ref in enumerate((r.egu.at[:, other], r.egu.at[:, other_up], r.ed.at[other])):
        arrived(ref, r.er.at[i])

    class Sums:
        up = square = branch = 0.0
        dense = [0.0, 0.0]

    def scaled_block(a, p):
        v = r.resid[a, p].reshape(tall, cols).astype(F32)
        return v, (v * r.gains[p]).astype(BF16)

    def absorb(sums, a, p):
        v, u = scaled_block(a, p)
        at = pl.ds(pl.multiple_of(p * cols, cols), cols)
        sums.square = sums.square + v * v
        sums.branch = sums.branch + u.astype(F32) * r.bgs[p]
        sums.up = sums.up + dot(u, r.egu[at])

    def absorb_dense(sums, a, p):
        u = scaled_block(a, p)[1]
        sums.dense = [d + dot_nt(u, r.sbuf1[c, p]) for c, d in enumerate(sums.dense)]

    first = Sums()
    absorb(first, xi, me)
    arrived(r.sbuf1.at[0, pl.ds(0, n - 1)], r.s1r.at[0])
    s_copies = [remote(r.sbuf1.at[core], r.sbuf1.at[core], r.ps.at[0], r.pr.at[0], me, pair)]
    s_copies[0].start()
    arrived(r.sbuf2.at[0, pl.ds(0, n - 1)], r.s2r.at[0])
    s_copies.append(
        remote(r.sbuf2.at[core], r.sbuf2.at[core], r.ps.at[1], r.pr.at[1], me, pair)
    )
    s_copies[1].start()
    for k in range(1, n // 2):
        arrived(r.resid.at[xi, peer(k)], r.fr.at[k])
        f_pass(k)
        absorb(first, xi, peer(k))
    arrived(r.sbuf1.at[0], r.pr.at[0])
    arrived(r.sbuf2.at[0], r.pr.at[1])
    for c in range(2):
        r.shared[c] = jnp.concatenate([r.sbuf2[c, e] for e in range(n)], axis=1)
    for k in range(n // 2):
        absorb_dense(first, xi, peer(k))
    for k in range(n // 2, n):
        arrived(r.resid.at[xi, peer(k)], r.fr.at[k])
        f_pass(k)
        absorb(first, xi, peer(k))
        absorb_dense(first, xi, peer(k))
    arrived(r.cbuf.at[pl.ds(0, n - 1)], r.cr.at[0])
    for a in range(half):
        for b in range(group):
            w = r.cbuf[b * m + 2 * a + core].astype(F32)
            r.routed[a, b * rows : (b + 1) * rows] = jnp.broadcast_to(
                w[:, 0:1] + w[:, 64:65], (rows, 128)
            )
    upper = me // (n // 2)

    def target(a, b):
        return b * m + 2 * a + core

    def away(a, b, q):
        return jnp.logical_or(target(a, b) != me, q != tp)

    def finish(sums, a):
        square = jnp.sum(sums.square, axis=1, keepdims=True)
        scale = lax.rsqrt(square / width + EPS)
        up = sums.up * scale
        act = (silu(up[:, : 2 * hidden]) * up[:, 2 * hidden :]).astype(BF16)
        dense = []
        for d in sums.dense:
            both = d * scale
            dense.append((silu(both[:, :units]) * both[:, units:]).astype(BF16))
        branch = sigmoid(jnp.sum(sums.branch, axis=1, keepdims=True) * scale)
        weight = r.routed[a, :, 0:1]
        for k in range(m):
            q = 2 * lax.rem(xi + k // 2, half) + lax.rem(core + k, 2)
            at = pl.ds(pl.multiple_of(q * quarter, quarter), quarter)
            out = weight * dot(act, r.ed[:, at])
            side = dot(dense[0], r.shared[0, :, at])
            side = side + dot(dense[1], r.shared[1, :, at])
            r.rsend[a, :, q] = (out + branch * side).astype(BF16).reshape(group, rows, quarter)
            for i in range(group):
                b = lax.rem(i + (group // 2) * (1 - upper), group)

                @pl.when(away(a, b, q))
                def _():
                    remote(
                        r.rsend.at[a, b, q],
                        r.rbuf.at[me * half + xi],
                        r.rs.at[0],
                        r.rr.at[0],
                        target(a, b),
                        q,
                    ).start()

    finish(first, xi)
    for i in range(1, half):
        a = lax.rem(xi + i, half)
        second = Sums()
        for g in range(2):
            arrived(r.resid.at[a, pl.ds(0, n // 2)], r.gr.at[a, g])
            for k in range(g * n // 2, (g + 1) * n // 2):
                absorb(second, a, peer(k))
                absorb_dense(second, a, peer(k))
        finish(second, a)

    held_here = core == lax.rem(home, 2)
    place = home // 2
    d_copy = remote(
        r.resid.at[place, pl.ds(pair * group, group), turn],
        r.rown,
        r.ds.at[0],
        r.dr.at[0],
        me,
        pair,
    )

    @pl.when(held_here)
    def _():
        d_copy.start()
        r.rown[...] = r.resid[place, pl.ds(tp * group, group), turn]
        r.rbuf[me * half + xi] = r.rsend[place, turn, tp]

    left(r.xbuf.at[pl.ds(0, n - 1)], r.xs.at[0])
    left(r.cbuf.at[pl.ds(0, n - 1)], r.cs.at[0])
    left(r.abuf.at[pl.ds(0, n - 1)], r.as_.at[0])
    left(r.part, r.us.at[0])
    left(r.vbuf.at[pl.ds(0, n // 2 - 1)], r.vs.at[0])
    left(r.sbuf1.at[0, pl.ds(0, n - 1)], r.s1s.at[0])
    left(r.sbuf2.at[0, pl.ds(0, n - 1)], r.s2s.at[0])
    left(r.resid.at[0, pl.ds(0, n - 1)], r.fs.at[0])
    if half > 1:
        left(r.resid.at[pl.ds(0, half - 1)], r.gs.at[0])
    left(r.wide_ow.at[pl.ds(0, (m - 1) * vc)], r.ows.at[0])
    for c in e_copies + s_copies:
        c.wait_send()

    @pl.when(at_home)
    def _():
        left(r.tsend.at[pl.ds(0, n - 1)], r.ts.at[0])
        left(r.hbuf.at[pl.ds(0, n - 1)], r.hs.at[0])

    @pl.when(jnp.logical_not(at_home))
    def _():
        left(r.hbuf, r.hs.at[0])

    @pl.when(held_here)
    def _():
        arrived(r.rbuf.at[pl.ds(0, n * half - 1)], r.rr.at[0])

    @pl.when(jnp.logical_not(held_here))
    def _():
        arrived(r.rbuf, r.rr.at[0])
        arrived(r.rown, r.dr.at[0])

    acc = jnp.concatenate([r.rown[b].astype(F32) for b in range(group)], axis=1)
    for p in range(n * half):
        acc = acc + r.rbuf[p].astype(F32)
    r.obuf[tp] = acc.astype(BF16)
    for i in range(1, m):
        t = lax.rem(tp + i, m)
        remote(r.obuf.at[tp], r.obuf.at[tp], r.os_.at[0], r.or_.at[0], me, t).start()

    @pl.when(held_here)
    def _():
        d_copy.wait_send()
        left(r.rbuf.at[pl.ds(0, n * half - 1)], r.rs.at[0])

    @pl.when(jnp.logical_not(held_here))
    def _():
        left(r.rbuf, r.rs.at[0])

    arrived(r.obuf.at[pl.ds(0, m - 1)], r.or_.at[0])
    for t in range(m):
        r.out[:, t * quarter : (t + 1) * quarter] = r.obuf[t]
    left(r.obuf.at[pl.ds(0, m - 1)], r.os_.at[0])


def flush_kernel(layer_ref, state_ref, layer_out, state_out, sem):
    rows = state_ref.shape[0]
    part = rows // STATE_PARTS
    copies = [pltpu.make_async_copy(layer_ref, layer_out, sem.at[STATE_PARTS])]
    for i in range(STATE_PARTS):
        these = pl.ds(i * part, part)
        copies.append(
            pltpu.make_async_copy(state_ref.at[these], state_out.at[these], sem.at[i])
        )
    for c in copies:
        c.start()
    for c in copies:
        c.wait()


VMEM = pl.BlockSpec(memory_space=pltpu.VMEM)
HBM = pl.BlockSpec(memory_space=pltpu.HBM)


def per_device(
    n,
    m,
    tokens,
    norm_gain,
    query_weight,
    key_weight,
    value_weight,
    outgate_weight,
    beta_weight,
    decay_weight,
    decay_rate,
    decay_bias,
    head_gain,
    recurrent,
    output_weight,
    ffn_gain,
    routes,
    route_weight,
    expert_gate,
    expert_up,
    expert_down,
    shared_gate,
    shared_up,
    shared_down,
    branch_gate,
):
    rows, width = tokens.shape
    _, heads, key_dim, value_dim = recurrent.shape
    depth, qc = query_weight.shape
    vc = value_weight.shape[1]
    keys = qc // key_dim
    total = 2 * qc + 2 * vc
    half = m // 2
    group = n // m
    units = shared_gate.shape[1] // n
    cols = shared_down.shape[1]
    hidden = expert_gate.shape[2]
    quarter = width // m
    sds = jax.ShapeDtypeStruct
    dma = pltpu.SemaphoreType.DMA

    inputs = dict(
        tokens=tokens,
        gain=norm_gain,
        qw=query_weight,
        kw=key_weight,
        vw=value_weight,
        gw=outgate_weight,
        beta=beta_weight.T,
        decay=decay_weight.T,
        rate=decay_rate[None, :],
        bias=decay_bias[None, :],
        routes=routes.T,
        rw=route_weight.T,
        head_gain=head_gain,
        state=recurrent,
        ow=output_weight,
        ffn_gain=ffn_gain,
        eg=expert_gate,
        eu=expert_up,
        ed=expert_down,
        sg=shared_gate,
        su=shared_up,
        sd=shared_down,
        bg=branch_gate,
    )
    plain = ("tokens", "gain", "beta", "decay", "rate", "bias", "routes", "rw")
    plain += ("head_gain", "ffn_gain", "sg", "su", "sd", "bg")
    scratch = {k: pltpu.VMEM(inputs[k].shape, inputs[k].dtype) for k in plain}
    scratch.update(
        weights=pltpu.VMEM((depth, total), BF16),
        wide_ow=pltpu.VMEM((m * vc, cols), BF16),
        egu=pltpu.VMEM((width, 4 * hidden), BF16),
        gains=pltpu.VMEM((n, 1, cols), F32),
        bgs=pltpu.VMEM((n, 1, cols), F32),
        ed=pltpu.VMEM((2 * hidden, width), BF16),
        xsend=pltpu.VMEM((n, rows, depth), BF16),
        xbuf=pltpu.VMEM((n, rows, depth), BF16),
        csend=pltpu.VMEM((n, rows, 128), BF16),
        cbuf=pltpu.VMEM((n, rows, 128), BF16),
        tsend=pltpu.VMEM((n, rows, depth), BF16),
        tbuf=pltpu.VMEM((group, rows, depth), BF16),
        ssend1=pltpu.VMEM((n, 2 * units, cols), BF16),
        sbuf1=pltpu.VMEM((2, n, 2 * units, cols), BF16),
        ssend2=pltpu.VMEM((n, units, cols), BF16),
        sbuf2=pltpu.VMEM((2, n, units, cols), BF16),
        shared=pltpu.VMEM((2, units, width), BF16),
        asend=pltpu.VMEM((n, rows, total), BF16),
        abuf=pltpu.VMEM((n, rows, 2 * qc), BF16),
        part=pltpu.VMEM((n // 2, rows, 2 * vc), BF16),
        vsend=pltpu.VMEM((n // 2, rows, 2 * vc), BF16),
        vbuf=pltpu.VMEM((n // 2, rows, 2 * vc), BF16),
        seen=pltpu.VMEM((rows, vc), F32),
        retain=pltpu.VMEM((rows, vc), F32),
        pull=pltpu.VMEM((rows, vc), F32),
        push=pltpu.VMEM((rows, vc), F32),
        qk=pltpu.VMEM((rows, keys * value_dim), F32),
        kq=pltpu.VMEM((key_dim, 128), F32),
        held=pltpu.VMEM((rows, vc), F32),
        routed=pltpu.VMEM((half, group * rows, 128), F32),
        hsend=pltpu.VMEM((rows, vc), BF16),
        hbuf=pltpu.VMEM((n, rows, vc), BF16),
        resid=pltpu.VMEM((half, n, group, rows, cols), BF16),
        rown=pltpu.VMEM((group, rows, cols), BF16),
        rsend=pltpu.VMEM((half, group, m, rows, quarter), BF16),
        rbuf=pltpu.VMEM((n * half, rows, quarter), BF16),
        obuf=pltpu.VMEM((m, rows, quarter), BF16),
        wsem=dma((len(inputs) - 5,)),
        psem=dma((2,)),
    )
    counts = dict(xr=4, ur=4, fr=n, es=3, er=3, ps=2, pr=2)
    for name in ("x", "c", "ow", "a", "u", "v", "t", "s1", "s2", "h", "f", "g", "e", "p", "d", "r", "o"):
        for end in ("s", "r"):
            key = {"as": "as_", "os": "os_", "or": "or_"}.get(name + end, name + end)
            scratch[key] = dma((counts.get(key, 1),))
    scratch["gr"] = dma((half, 2))
    names = [k + "_hbm" for k in inputs] + ["out", "new"] + list(scratch)
    layer, state = pl.pallas_call(
        functools.partial(layer_kernel, n, m, names),
        out_shape=(pltpu.VMEM((rows, width), BF16), pltpu.VMEM(recurrent.shape, F32)),
        in_specs=[HBM] * len(inputs),
        out_specs=(VMEM, VMEM),
        scratch_shapes=list(scratch.values()),
        compiler_params=pltpu.CompilerParams(
            collective_id=0, has_side_effects=True, vmem_limit_bytes=48 * 2**20
        ),
    )(*(pltpu.with_memory_space_constraint(v, pltpu.HBM) for v in inputs.values()))

    return pl.pallas_call(
        flush_kernel,
        out_shape=(sds((rows, width), BF16), sds(recurrent.shape, F32)),
        in_specs=[VMEM, VMEM],
        out_specs=(HBM, HBM),
        scratch_shapes=[dma((STATE_PARTS + 1,))],
        compiler_params=pltpu.CompilerParams(vmem_limit_bytes=4 * 2**20),
    )(layer, state)


def solution(mesh):
    return jax.shard_map(
        functools.partial(per_device, mesh.shape["ep"], mesh.shape["tp"]),
        mesh=mesh,
        in_specs=(
            P("ep", None),
            P(),
            P("ep", "tp"),
            P("ep", "tp"),
            P("ep", "tp"),
            P("ep", "tp"),
            P(),
            P(),
            P("tp"),
            P("tp"),
            P(),
            P("ep", "tp", None, None),
            P("tp", "ep"),
            P(),
            P("ep", None),
            P("ep", None),
            P("ep", None, "tp"),
            P("ep", None, "tp"),
            P("ep", "tp", None),
            P("ep", "tp"),
            P("ep", "tp"),
            P("tp", "ep"),
            P(),
        ),
        out_specs=(P("ep", None), P("ep", "tp", None, None)),
        check_vma=False,
    )
```

```python
import functools
import types

import jax
import jax.numpy as jnp
from jax import lax
from jax.experimental import pallas as pl
from jax.experimental.pallas import tpu as pltpu
from jax.sharding import PartitionSpec as P

EPS = 1e-06
ROUTED_SCALE = 2.5
MESH = pl.DeviceIdType.MESH
F32 = jnp.float32
BF16 = jnp.bfloat16
STATE_PARTS = 4


def silu(v):
    return v / (1.0 + jnp.exp(-v))


def sigmoid(v):
    return 1.0 / (1.0 + jnp.exp(-v))


def rms_scale(values, gain):
    values = values.astype(F32)
    return (
        values
        * lax.rsqrt(jnp.mean(values * values, axis=-1, keepdims=True) + EPS)
        * gain.astype(F32).reshape(1, -1)
    )


def unit_rows(values):
    return values * lax.rsqrt(jnp.sum(values * values, axis=-1, keepdims=True) + EPS)


def dot(a, b):
    return jnp.dot(a, b, preferred_element_type=F32)


def dot_nt(a, b):
    return lax.dot_general(a, b, (((1,), (1,)), ((), ())), preferred_element_type=F32)


def remote(src, dst, send_sem, recv_sem, e, t):
    return pltpu.make_async_remote_copy(
        src_ref=src,
        dst_ref=dst,
        send_sem=send_sem,
        recv_sem=recv_sem,
        device_id=(e, t),
        device_id_type=MESH,
    )


def loop(lo, hi, body):
    def step(i, c):
        body(i)
        return c

    lax.fori_loop(lo, hi, step, 0)


def layer_kernel(n, m, names, *refs):
    r = types.SimpleNamespace(**dict(zip(names, refs)))
    me, tp = lax.axis_index("ep"), lax.axis_index("tp")
    half = m // 2
    group = n // m
    core = lax.rem(tp, 2)
    pair = tp + 1 - 2 * core
    xi = tp // 2
    home = lax.rem(me, m)
    turn = me // m
    rows, width = r.tokens.shape
    depth, qc = r.qw_hbm.shape
    vc = r.vw_hbm.shape[1]
    key_dim, value_dim = r.new.shape[2], r.new.shape[3]
    heads = r.new.shape[1]
    keys = qc // key_dim
    share = heads // keys
    total = 2 * qc + 2 * vc
    cols = r.wide_ow.shape[1]
    hidden = r.eg_hbm.shape[2]
    quarter = width // m
    units = r.ssend2.shape[1]
    tall = group * rows

    barrier = pltpu.get_barrier_semaphore()

    steps = [
        (1 - 2 * lax.rem(me // 2**i, 2)) * 2**i for i in range(n.bit_length() - 1)
    ]

    def peer(k):
        p = me
        for i, step in enumerate(steps):
            if k >> i & 1:
                p = p + step
        return p

    cuts = (n // 2, 3 * n // 4, n), (n // 4, n // 2), (0, n // 4)
    spans = [cuts[0][:2], cuts[0][1:], cuts[1], cuts[2]]
    order = [k for lo, hi in spans for k in range(lo, hi) if k]

    for k in order:
        pl.semaphore_signal(barrier, inc=1, device_id=(peer(k), tp), device_id_type=MESH)
    for i in range(1, m):
        pl.semaphore_signal(
            barrier, inc=1, device_id=(me, lax.rem(tp + i, m)), device_id_type=MESH
        )

    fetches, alone = {}, []

    def fetch(name, src, dst, sem=None):
        if sem is None:
            sem = r.wsem.at[len(alone)]
            alone.append(name)
        c = pltpu.make_async_copy(src, dst, sem)
        c.start()
        fetches[name] = c

    for name in ("tokens", "gain"):
        fetch(name, getattr(r, name + "_hbm"), getattr(r, name))
    at = 0
    for name in ("qw", "kw", "vw", "gw"):
        src = getattr(r, name + "_hbm")
        fetch(name, src, r.weights.at[:, pl.ds(at, src.shape[1])], r.psem.at[0])
        at += src.shape[1]
    for name in ("routes", "rw", "sd", "beta", "decay", "rate", "bias", "sg", "su"):
        fetch(name, getattr(r, name + "_hbm"), getattr(r, name))
    part = rows // STATE_PARTS
    for i in range(STATE_PARTS):
        these = pl.ds(i * part, part)
        fetch(("state", i), r.state_hbm.at[these], r.new.at[these], r.psem.at[1])
    for name in ("head_gain", "ffn_gain", "bg"):
        fetch(name, getattr(r, name + "_hbm"), getattr(r, name))
    own_ow = pl.ds(pl.multiple_of(tp * vc, vc), vc)
    mine = pl.ds(pl.multiple_of(core * hidden, hidden), hidden)
    other = pl.ds(pl.multiple_of((1 - core) * hidden, hidden), hidden)
    fetch("ow", r.ow_hbm, r.wide_ow.at[own_ow])
    mine_up = pl.ds(pl.multiple_of((2 + core) * hidden, hidden), hidden)
    other_up = pl.ds(pl.multiple_of((3 - core) * hidden, hidden), hidden)
    fetch("eg", r.eg_hbm.at[0], r.egu.at[:, mine])
    fetch("eu", r.eu_hbm.at[0], r.egu.at[:, mine_up])
    fetch("ed", r.ed_hbm.at[0], r.ed.at[mine])

    def arrived(ref, sem):
        remote(ref, ref, sem, sem, me, pair).wait_recv()

    def left(ref, sem):
        remote(ref, ref, sem, sem, me, pair).wait_send()

    fetches["tokens"].wait()
    fetches["gain"].wait()
    tokens = r.tokens[...]
    normed = rms_scale(tokens, r.gain[...]).astype(BF16)
    for e in range(n):
        r.xsend[e] = normed[:, e * depth : (e + 1) * depth]
        r.tsend[e] = tokens[:, e * depth : (e + 1) * depth]

    fetches["routes"].wait()
    fetches["rw"].wait()
    rw = r.rw[...]
    scaled = rw / jnp.sum(rw, axis=0, keepdims=True) * ROUTED_SCALE
    routes = r.routes[...]
    expert = lax.broadcasted_iota(jnp.int32, (128, rows), 0)
    by_expert = jnp.zeros((128, rows), F32)
    for k in range(routes.shape[0]):
        by_expert = by_expert + jnp.where(
            expert == routes[k : k + 1, :], scaled[k : k + 1, :], 0.0
        )
    by_expert = by_expert.T
    lane = lax.broadcasted_iota(jnp.int32, (rows, 128), 1)
    for e in range(n):
        w = by_expert[:, e : e + 1]
        high = w.astype(BF16).astype(F32)
        r.csend[e] = jnp.where(lane < 64, high, w - high).astype(BF16)
    fetches["sd"].wait()
    for e in range(n):
        r.ssend2[e] = r.sd[e * units : (e + 1) * units]
    pl.semaphore_wait(barrier, n + m - 2)

    for g, (lo, hi) in enumerate(spans):
        for k in range(max(lo, 1), hi):
            p = peer(k)
            remote(r.xsend.at[p], r.xbuf.at[k], r.xs.at[0], r.xr.at[g], p, tp).start()
    r.xbuf[0] = r.xsend[me]
    def send_shared(src, dst, s, d):
        for k in order:
            p = peer(k)
            remote(src.at[p], dst.at[core, me], s.at[0], d.at[0], p, tp).start()
        dst[core, me] = src[me]

    send_shared(r.ssend2, r.sbuf2, r.s2s, r.s2r)

    for i in range(1, m):
        t = lax.rem(tp + i, m)
        remote(r.ow_hbm, r.wide_ow.at[own_ow], r.ows.at[0], r.owr.at[0], me, t).start()
    e_copies = [
        remote(r.eg_hbm.at[0], r.egu.at[:, mine], r.es.at[0], r.er.at[0], me, pair),
        remote(r.eu_hbm.at[0], r.egu.at[:, mine_up], r.es.at[1], r.er.at[1], me, pair),
        remote(r.ed_hbm.at[0], r.ed.at[mine], r.es.at[2], r.er.at[2], me, pair),
    ]
    for c in e_copies:
        c.start()

    for name in ("beta", "decay", "rate", "bias", "sg", "su"):
        fetches[name].wait()
    place_of = lax.broadcasted_iota(jnp.int32, (rows, r.beta.shape[0]), 1)

    def own_heads(w):
        logits = dot_nt(normed, w)
        return [
            jnp.sum(jnp.where(place_of == tp * heads + h, logits, 0.0), axis=1, keepdims=True)
            for h in range(heads)
        ]

    def wide(v):
        return jnp.broadcast_to(v, (rows, value_dim))

    beta = own_heads(r.beta[...])
    decay = own_heads(r.decay[...])
    for h in range(heads):
        at = slice(h * value_dim, (h + 1) * value_dim)
        strength = sigmoid(wide(beta[h]))
        shifted = wide(decay[h]) + r.bias[:, h : h + 1]
        softplus = jnp.maximum(shifted, 0.0) + jnp.log1p(jnp.exp(-jnp.abs(shifted)))
        retain = jnp.exp(-r.rate[:, h : h + 1] * softplus)
        r.retain[:, at] = retain
        r.pull[:, at] = strength * retain
        r.push[:, at] = strength
    for at, name in enumerate(("sg", "su")):
        by_unit = getattr(r, name)[...].astype(F32).T.astype(BF16)
        for e in range(n):
            r.ssend1[e, at * units : (at + 1) * units] = by_unit[e * units : (e + 1) * units]

    pltpu.make_async_copy(r.weights, r.weights, r.psem.at[0]).wait()
    for g, (lo, hi) in reversed(list(enumerate(spans))):
        if hi > max(lo, 1):
            arrived(r.xbuf.at[pl.ds(max(lo, 1), hi - max(lo, 1))], r.xr.at[g])
        x = r.xbuf[lo:hi].reshape((hi - lo) * rows, depth)
        for c in range(0, total, 512):
            size = min(512, total - c)
            out = dot(x, r.weights[:, c : c + size])
            r.asend[lo:hi, :, c : c + size] = out.astype(BF16).reshape(hi - lo, rows, size)
        for k in range(lo + 1, hi, 2):
            remote(
                r.asend.at[k, :, pl.ds(2 * qc, 2 * vc)],
                r.part.at[k // 2],
                r.us.at[0],
                r.ur.at[g],
                peer(1),
                tp,
            ).start()
        for k in range(max(lo, 1), hi):
            remote(
                r.asend.at[k, :, pl.ds(0, 2 * qc)],
                r.abuf.at[k],
                r.as_.at[0],
                r.ar.at[0],
                peer(k),
                tp,
            ).start()
    r.abuf[0] = r.asend[0, :, : 2 * qc]

    at_home = tp == home

    @pl.when(at_home)
    def _():
        for k in order:
            p = peer(k)
            remote(
                r.tsend.at[p], r.tbuf.at[turn], r.ts.at[0], r.tr.at[0], p, tp
            ).start()
        r.tbuf[turn] = r.tsend[me]

    for g, (lo, hi) in reversed(list(enumerate(spans))):
        arrived(r.part.at[pl.ds(lo // 2, (hi - lo) // 2)], r.ur.at[g])
        for k in range(lo // 2, hi // 2):
            own = r.asend[2 * k, :, 2 * qc :].astype(F32)
            both = (own + r.part[k].astype(F32)).astype(BF16)
            if k == 0:
                r.vbuf[0] = both
            else:
                r.vsend[k] = both
                remote(
                    r.vsend.at[k], r.vbuf.at[k], r.vs.at[0], r.vr.at[0], peer(2 * k), tp
                ).start()

    for name in ("head_gain", "ffn_gain", "bg"):
        fetches[name].wait()
    gain = r.ffn_gain[...].astype(F32).reshape(1, -1)
    bg = r.bg[...].astype(F32).reshape(1, -1)
    for e in range(n):
        r.gains[e] = gain[:, e * cols : (e + 1) * cols]
        r.bgs[e] = bg[:, e * cols : (e + 1) * cols]
    pltpu.make_async_copy(r.new, r.new, r.psem.at[1]).wait()

    arrived(r.abuf.at[pl.ds(1, n - 1)], r.ar.at[0])

    def gathered(ref, c, size):
        acc = ref[0, :, c : c + size].astype(F32)
        for e in range(1, ref.shape[0]):
            acc = acc + ref[e, :, c : c + size].astype(F32)
        return acc.astype(BF16).astype(F32)

    q_rows = [
        unit_rows(silu(gathered(r.abuf, j * key_dim, key_dim))) * key_dim ** (-0.5)
        for j in range(keys)
    ]
    k_rows = [
        unit_rows(silu(gathered(r.abuf, qc + j * key_dim, key_dim))) for j in range(keys)
    ]
    for j in range(keys):
        r.qk[:, j * value_dim : (j + 1) * value_dim] = wide(
            jnp.sum(q_rows[j] * k_rows[j], axis=1, keepdims=True)
        )
    stacked = q_rows + k_rows
    stacked.append(jnp.zeros((128 - 2 * keys * rows, key_dim), F32))
    r.kq[...] = jnp.concatenate(stacked, axis=0).T

    def column(at):
        return jnp.broadcast_to(r.kq[:, at : at + 1], (key_dim, value_dim))

    for j in range(keys):
        for s in range(rows):
            q, k = column(j * rows + s), column((keys + j) * rows + s)
            for h in range(j * share, (j + 1) * share):
                c = slice(h * value_dim, (h + 1) * value_dim)
                state = r.new[s, h]
                r.seen[s : s + 1, c] = jnp.sum(state * k, axis=0, keepdims=True)
                r.held[s : s + 1, c] = jnp.sum(state * q, axis=0, keepdims=True)

    arrived(r.vbuf.at[pl.ds(1, n // 2 - 1)], r.vr.at[0])
    for h in range(heads):
        c = slice(h * value_dim, (h + 1) * value_dim)
        j = h // share
        values = silu(gathered(r.vbuf, h * value_dim, value_dim))
        gate = silu(gathered(r.vbuf, vc + h * value_dim, value_dim))
        correction = r.push[:, c] * values - r.pull[:, c] * r.seen[:, c]
        r.seen[:, c] = correction
        qk = r.qk[:, j * value_dim : (j + 1) * value_dim]
        readout = r.held[:, c] * r.retain[:, c] + qk * correction
        r.hsend[:, c] = (rms_scale(readout, r.head_gain[...]) * gate).astype(BF16)

    def send_h(p):
        remote(
            r.hsend, r.hbuf.at[turn * m + tp], r.hs.at[0], r.hr.at[tp], p, home
        ).start()

    for k in order:
        send_h(peer(k))

    @pl.when(jnp.logical_not(at_home))
    def _():
        send_h(me)

    @pl.when(at_home)
    def _():
        r.hbuf[turn * m + tp] = r.hsend[...]

    send_shared(r.ssend1, r.sbuf1, r.s1s, r.s1r)
    for k in order:
        p = peer(k)
        remote(r.csend.at[p], r.cbuf.at[me], r.cs.at[0], r.cr.at[0], p, tp).start()
    r.cbuf[me] = r.csend[me]

    for j in range(keys):
        for s in range(rows):
            k = column((keys + j) * rows + s)
            for h in range(j * share, (j + 1) * share):
                c = slice(h * value_dim, (h + 1) * value_dim)
                r.new[s, h] = (
                    r.new[s, h] * r.retain[s : s + 1, c] + k * r.seen[s : s + 1, c]
                )

    fetches["ow"].wait()
    arrived(r.wide_ow.at[pl.ds(0, (m - 1) * vc)], r.owr.at[0])

    @pl.when(at_home)
    def _():
        arrived(r.tbuf.at[pl.ds(0, group - 1)], r.tr.at[0])
        arrived(r.hbuf.at[pl.ds(0, group - 1)], r.hr.at[tp])

    @pl.when(jnp.logical_not(at_home))
    def _():
        arrived(r.tbuf, r.tr.at[0])
        arrived(r.hbuf.at[pl.ds(0, group)], r.hr.at[tp])

    residual = r.tbuf[...].reshape(tall, cols).astype(F32)
    mix = None
    for i in range(m):
        t = 2 * lax.rem(xi + i // 2, half) + lax.rem(core + i, 2)
        if i:
            arrived(r.hbuf.at[pl.ds(0, group)], r.hr.at[t])
        h = jnp.concatenate([r.hbuf[b * m + t] for b in range(group)], axis=0)
        term = dot(h, r.wide_ow[pl.ds(pl.multiple_of(t * vc, vc), vc)])
        mix = term if mix is None else mix + term
    r.resid[xi, me] = (residual + mix).astype(BF16).reshape(group, rows, cols)

    mine_resid = r.resid.at[xi, me]
    for k in order:
        remote(mine_resid, mine_resid, r.fs.at[0], r.fr.at[k], peer(k), tp).start()

    def f_pass(k):
        ref = r.resid.at[xi, peer(k)]
        sem = r.gr.at[xi, 2 * k // n]
        for i in range(1, half):
            t = 2 * lax.rem(xi + i, half) + core
            remote(ref, ref, r.gs.at[0], sem, me, t).start()

    f_pass(0)

    for name in ("eg", "eu", "ed"):
        fetches[name].wait()
    for i, ref in enumerate((r.egu.at[:, other], r.egu.at[:, other_up], r.ed.at[other])):
        arrived(ref, r.er.at[i])

    class Sums:
        up = square = branch = 0.0
        dense = [0.0, 0.0]

    def scaled_block(a, p):
        v = r.resid[a, p].reshape(tall, cols).astype(F32)
        return v, (v * r.gains[p]).astype(BF16)

    def absorb(sums, a, p):
        v, u = scaled_block(a, p)
        at = pl.ds(pl.multiple_of(p * cols, cols), cols)
        sums.square = sums.square + v * v
        sums.branch = sums.branch + u.astype(F32) * r.bgs[p]
        sums.up = sums.up + dot(u, r.egu[at])

    def absorb_dense(sums, a, p):
        u = scaled_block(a, p)[1]
        sums.dense = [d + dot_nt(u, r.sbuf1[c, p]) for c, d in enumerate(sums.dense)]

    first = Sums()
    absorb(first, xi, me)
    arrived(r.sbuf1.at[0, pl.ds(0, n - 1)], r.s1r.at[0])
    s_copies = [remote(r.sbuf1.at[core], r.sbuf1.at[core], r.ps.at[0], r.pr.at[0], me, pair)]
    s_copies[0].start()
    arrived(r.sbuf2.at[0, pl.ds(0, n - 1)], r.s2r.at[0])
    s_copies.append(
        remote(r.sbuf2.at[core], r.sbuf2.at[core], r.ps.at[1], r.pr.at[1], me, pair)
    )
    s_copies[1].start()
    for k in range(1, n // 2):
        arrived(r.resid.at[xi, peer(k)], r.fr.at[k])
        f_pass(k)
        absorb(first, xi, peer(k))
    arrived(r.sbuf1.at[0], r.pr.at[0])
    arrived(r.sbuf2.at[0], r.pr.at[1])
    for c in range(2):
        r.shared[c] = jnp.concatenate([r.sbuf2[c, e] for e in range(n)], axis=1)
    for k in range(n // 2):
        absorb_dense(first, xi, peer(k))
    for k in range(n // 2, n):
        arrived(r.resid.at[xi, peer(k)], r.fr.at[k])
        f_pass(k)
        absorb(first, xi, peer(k))
        absorb_dense(first, xi, peer(k))
    arrived(r.cbuf.at[pl.ds(0, n - 1)], r.cr.at[0])
    for a in range(half):
        for b in range(group):
            w = r.cbuf[b * m + 2 * a + core].astype(F32)
            r.routed[a, b * rows : (b + 1) * rows] = jnp.broadcast_to(
                w[:, 0:1] + w[:, 64:65], (rows, 128)
            )
    upper = me // (n // 2)

    def target(a, b):
        return b * m + 2 * a + core

    def away(a, b, q):
        return jnp.logical_or(target(a, b) != me, q != tp)

    def finish(sums, a):
        square = jnp.sum(sums.square, axis=1, keepdims=True)
        scale = lax.rsqrt(square / width + EPS)
        up = sums.up * scale
        act = (silu(up[:, : 2 * hidden]) * up[:, 2 * hidden :]).astype(BF16)
        dense = []
        for d in sums.dense:
            both = d * scale
            dense.append((silu(both[:, :units]) * both[:, units:]).astype(BF16))
        branch = sigmoid(jnp.sum(sums.branch, axis=1, keepdims=True) * scale)
        weight = r.routed[a, :, 0:1]
        for k in range(m):
            q = 2 * lax.rem(xi + k // 2, half) + lax.rem(core + k, 2)
            at = pl.ds(pl.multiple_of(q * quarter, quarter), quarter)
            out = weight * dot(act, r.ed[:, at])
            side = dot(dense[0], r.shared[0, :, at])
            side = side + dot(dense[1], r.shared[1, :, at])
            r.rsend[a, :, q] = (out + branch * side).astype(BF16).reshape(group, rows, quarter)
            for i in range(group):
                b = lax.rem(i + (group // 2) * (1 - upper), group)

                @pl.when(away(a, b, q))
                def _():
                    remote(
                        r.rsend.at[a, b, q],
                        r.rbuf.at[me * half + xi],
                        r.rs.at[0],
                        r.rr.at[0],
                        target(a, b),
                        q,
                    ).start()

    finish(first, xi)
    for i in range(1, half):
        a = lax.rem(xi + i, half)
        second = Sums()
        for g in range(2):
            arrived(r.resid.at[a, pl.ds(0, n // 2)], r.gr.at[a, g])
            for k in range(g * n // 2, (g + 1) * n // 2):
                absorb(second, a, peer(k))
                absorb_dense(second, a, peer(k))
        finish(second, a)

    held_here = core == lax.rem(home, 2)
    place = home // 2
    d_copy = remote(
        r.resid.at[place, pl.ds(pair * group, group), turn],
        r.rown,
        r.ds.at[0],
        r.dr.at[0],
        me,
        pair,
    )

    @pl.when(held_here)
    def _():
        d_copy.start()
        r.rown[...] = r.resid[place, pl.ds(tp * group, group), turn]
        r.rbuf[me * half + xi] = r.rsend[place, turn, tp]

    left(r.xbuf.at[pl.ds(0, n - 1)], r.xs.at[0])
    left(r.cbuf.at[pl.ds(0, n - 1)], r.cs.at[0])
    left(r.abuf.at[pl.ds(0, n - 1)], r.as_.at[0])
    left(r.part, r.us.at[0])
    left(r.vbuf.at[pl.ds(0, n // 2 - 1)], r.vs.at[0])
    left(r.sbuf1.at[0, pl.ds(0, n - 1)], r.s1s.at[0])
    left(r.sbuf2.at[0, pl.ds(0, n - 1)], r.s2s.at[0])
    left(r.resid.at[0, pl.ds(0, n - 1)], r.fs.at[0])
    if half > 1:
        left(r.resid.at[pl.ds(0, half - 1)], r.gs.at[0])
    left(r.wide_ow.at[pl.ds(0, (m - 1) * vc)], r.ows.at[0])
    for c in e_copies + s_copies:
        c.wait_send()

    @pl.when(at_home)
    def _():
        left(r.tsend.at[pl.ds(0, n - 1)], r.ts.at[0])
        left(r.hbuf.at[pl.ds(0, n - 1)], r.hs.at[0])

    @pl.when(jnp.logical_not(at_home))
    def _():
        left(r.hbuf, r.hs.at[0])

    @pl.when(held_here)
    def _():
        arrived(r.rbuf.at[pl.ds(0, n * half - 1)], r.rr.at[0])

    @pl.when(jnp.logical_not(held_here))
    def _():
        arrived(r.rbuf, r.rr.at[0])
        arrived(r.rown, r.dr.at[0])

    acc = jnp.concatenate([r.rown[b].astype(F32) for b in range(group)], axis=1)
    for p in range(n * half):
        acc = acc + r.rbuf[p].astype(F32)
    r.obuf[tp] = acc.astype(BF16)
    for i in range(1, m):
        t = lax.rem(tp + i, m)
        remote(r.obuf.at[tp], r.obuf.at[tp], r.os_.at[0], r.or_.at[0], me, t).start()

    @pl.when(held_here)
    def _():
        d_copy.wait_send()
        left(r.rbuf.at[pl.ds(0, n * half - 1)], r.rs.at[0])

    @pl.when(jnp.logical_not(held_here))
    def _():
        left(r.rbuf, r.rs.at[0])

    arrived(r.obuf.at[pl.ds(0, m - 1)], r.or_.at[0])
    for t in range(m):
        r.out[:, t * quarter : (t + 1) * quarter] = r.obuf[t]
    left(r.obuf.at[pl.ds(0, m - 1)], r.os_.at[0])


def flush_kernel(layer_ref, state_ref, layer_out, state_out, sem):
    rows = state_ref.shape[0]
    part = rows // STATE_PARTS
    copies = [pltpu.make_async_copy(layer_ref, layer_out, sem.at[STATE_PARTS])]
    for i in range(STATE_PARTS):
        these = pl.ds(i * part, part)
        copies.append(
            pltpu.make_async_copy(state_ref.at[these], state_out.at[these], sem.at[i])
        )
    for c in copies:
        c.start()
    for c in copies:
        c.wait()


VMEM = pl.BlockSpec(memory_space=pltpu.VMEM)
HBM = pl.BlockSpec(memory_space=pltpu.HBM)


def per_device(
    n,
    m,
    tokens,
    norm_gain,
    query_weight,
    key_weight,
    value_weight,
    outgate_weight,
    beta_weight,
    decay_weight,
    decay_rate,
    decay_bias,
    head_gain,
    recurrent,
    output_weight,
    ffn_gain,
    routes,
    route_weight,
    expert_gate,
    expert_up,
    expert_down,
    shared_gate,
    shared_up,
    shared_down,
    branch_gate,
):
    rows, width = tokens.shape
    _, heads, key_dim, value_dim = recurrent.shape
    depth, qc = query_weight.shape
    vc = value_weight.shape[1]
    keys = qc // key_dim
    total = 2 * qc + 2 * vc
    half = m // 2
    group = n // m
    units = shared_gate.shape[1] // n
    cols = shared_down.shape[1]
    hidden = expert_gate.shape[2]
    quarter = width // m
    sds = jax.ShapeDtypeStruct
    dma = pltpu.SemaphoreType.DMA

    inputs = dict(
        tokens=tokens,
        gain=norm_gain,
        qw=query_weight,
        kw=key_weight,
        vw=value_weight,
        gw=outgate_weight,
        beta=beta_weight.T,
        decay=decay_weight.T,
        rate=decay_rate[None, :],
        bias=decay_bias[None, :],
        routes=routes.T,
        rw=route_weight.T,
        head_gain=head_gain,
        state=recurrent,
        ow=output_weight,
        ffn_gain=ffn_gain,
        eg=expert_gate,
        eu=expert_up,
        ed=expert_down,
        sg=shared_gate,
        su=shared_up,
        sd=shared_down,
        bg=branch_gate,
    )
    plain = ("tokens", "gain", "beta", "decay", "rate", "bias", "routes", "rw")
    plain += ("head_gain", "ffn_gain", "sg", "su", "sd", "bg")
    scratch = {k: pltpu.VMEM(inputs[k].shape, inputs[k].dtype) for k in plain}
    scratch.update(
        weights=pltpu.VMEM((depth, total), BF16),
        wide_ow=pltpu.VMEM((m * vc, cols), BF16),
        egu=pltpu.VMEM((width, 4 * hidden), BF16),
        gains=pltpu.VMEM((n, 1, cols), F32),
        bgs=pltpu.VMEM((n, 1, cols), F32),
        ed=pltpu.VMEM((2 * hidden, width), BF16),
        xsend=pltpu.VMEM((n, rows, depth), BF16),
        xbuf=pltpu.VMEM((n, rows, depth), BF16),
        csend=pltpu.VMEM((n, rows, 128), BF16),
        cbuf=pltpu.VMEM((n, rows, 128), BF16),
        tsend=pltpu.VMEM((n, rows, depth), BF16),
        tbuf=pltpu.VMEM((group, rows, depth), BF16),
        ssend1=pltpu.VMEM((n, 2 * units, cols), BF16),
        sbuf1=pltpu.VMEM((2, n, 2 * units, cols), BF16),
        ssend2=pltpu.VMEM((n, units, cols), BF16),
        sbuf2=pltpu.VMEM((2, n, units, cols), BF16),
        shared=pltpu.VMEM((2, units, width), BF16),
        asend=pltpu.VMEM((n, rows, total), BF16),
        abuf=pltpu.VMEM((n, rows, 2 * qc), BF16),
        part=pltpu.VMEM((n // 2, rows, 2 * vc), BF16),
        vsend=pltpu.VMEM((n // 2, rows, 2 * vc), BF16),
        vbuf=pltpu.VMEM((n // 2, rows, 2 * vc), BF16),
        seen=pltpu.VMEM((rows, vc), F32),
        retain=pltpu.VMEM((rows, vc), F32),
        pull=pltpu.VMEM((rows, vc), F32),
        push=pltpu.VMEM((rows, vc), F32),
        qk=pltpu.VMEM((rows, keys * value_dim), F32),
        kq=pltpu.VMEM((key_dim, 128), F32),
        held=pltpu.VMEM((rows, vc), F32),
        routed=pltpu.VMEM((half, group * rows, 128), F32),
        hsend=pltpu.VMEM((rows, vc), BF16),
        hbuf=pltpu.VMEM((n, rows, vc), BF16),
        resid=pltpu.VMEM((half, n, group, rows, cols), BF16),
        rown=pltpu.VMEM((group, rows, cols), BF16),
        rsend=pltpu.VMEM((half, group, m, rows, quarter), BF16),
        rbuf=pltpu.VMEM((n * half, rows, quarter), BF16),
        obuf=pltpu.VMEM((m, rows, quarter), BF16),
        wsem=dma((len(inputs) - 5,)),
        psem=dma((2,)),
    )
    counts = dict(xr=4, hr=m, ur=4, fr=n, es=3, er=3, ps=2, pr=2)
    for name in ("x", "c", "ow", "a", "u", "v", "t", "s1", "s2", "h", "f", "g", "e", "p", "d", "r", "o"):
        for end in ("s", "r"):
            key = {"as": "as_", "os": "os_", "or": "or_"}.get(name + end, name + end)
            scratch[key] = dma((counts.get(key, 1),))
    scratch["gr"] = dma((half, 2))
    names = [k + "_hbm" for k in inputs] + ["out", "new"] + list(scratch)
    layer, state = pl.pallas_call(
        functools.partial(layer_kernel, n, m, names),
        out_shape=(pltpu.VMEM((rows, width), BF16), pltpu.VMEM(recurrent.shape, F32)),
        in_specs=[HBM] * len(inputs),
        out_specs=(VMEM, VMEM),
        scratch_shapes=list(scratch.values()),
        compiler_params=pltpu.CompilerParams(
            collective_id=0, has_side_effects=True, vmem_limit_bytes=48 * 2**20
        ),
    )(*(pltpu.with_memory_space_constraint(v, pltpu.HBM) for v in inputs.values()))

    return pl.pallas_call(
        flush_kernel,
        out_shape=(sds((rows, width), BF16), sds(recurrent.shape, F32)),
        in_specs=[VMEM, VMEM],
        out_specs=(HBM, HBM),
        scratch_shapes=[dma((STATE_PARTS + 1,))],
        compiler_params=pltpu.CompilerParams(vmem_limit_bytes=4 * 2**20),
    )(layer, state)


def solution(mesh):
    return jax.shard_map(
        functools.partial(per_device, mesh.shape["ep"], mesh.shape["tp"]),
        mesh=mesh,
        in_specs=(
            P("ep", None),
            P(),
            P("ep", "tp"),
            P("ep", "tp"),
            P("ep", "tp"),
            P("ep", "tp"),
            P(),
            P(),
            P("tp"),
            P("tp"),
            P(),
            P("ep", "tp", None, None),
            P("tp", "ep"),
            P(),
            P("ep", None),
            P("ep", None),
            P("ep", None, "tp"),
            P("ep", None, "tp"),
            P("ep", "tp", None),
            P("ep", "tp"),
            P("ep", "tp"),
            P("tp", "ep"),
            P(),
        ),
        out_specs=(P("ep", None), P("ep", "tp", None, None)),
        check_vma=False,
    )
```
